32 devices in a mesh: sp: 8 (over z, y), tp: 4 (over x, core).
Axes of the slice: x: 2, y: 2, z: 4, core: 2. Of those that a mesh axis runs over, the one named last changes fastest.
Arguments:
- stream: bfloat16 [1536, 2048], P('sp'), may hold values from -6 to 6
- upstream: bfloat16 [1536, 2048], P('sp'), may hold values from -6 to 6
- expert_gain: float32 [2048], replicated, may hold values from 0.1 to 1.9
- expert_ids: int32 [1536, 2], P('sp'), may hold values from 0 to 7, all different within a row; in each aligned block of 192 rows (0 to 191, 192 to 383, ...) at most 60 rows name the same one
- group_weight: float32 [1536], P('sp'), may hold values from 0.25 to 1
- pair_scores: float32 [1536, 2], P('sp'), may hold values from -6 to 6
- gate_weight: bfloat16 [8, 2048, 1024], P('sp', None, 'tp'), may hold values from -0.125 to 0.125
- up_weight: bfloat16 [8, 2048, 1024], P('sp', None, 'tp'), may hold values from -0.125 to 0.125
- down_weight: bfloat16 [8, 1024, 2048], P('sp', 'tp'), may hold values from -0.1875 to 0.1875
- mixer_weight: bfloat16 [1024, 2048], P('tp'), may hold values from -0.1875 to 0.1875
- filtered: bfloat16 [1536, 1024], P('sp', 'tp'), may hold values from -1000 to 1000
- channel_gain: float32 [1024], P('tp'), may hold values from 0.1 to 1.9
- kernel_taps: float32 [31, 1024], P(None, 'tp'), may hold values from -1 to 1
- value_branch: bfloat16 [1536, 1024], P('sp', 'tp'), may hold values from -6 to 6
- gate_branch: bfloat16 [1536, 1024], P('sp', 'tp'), may hold values from -6 to 6
Outputs:
- gradient_value: bfloat16 [1536, 1024], P('sp', 'tp')
- gradient_gating: bfloat16 [1536, 1024], P('sp', 'tp')
- gradient_mixer: float32 [2048, 1024], P('sp', 'tp')
- gradient_gate: float32 [8, 2048, 1024], P('sp', None, 'tp')
- gradient_up: float32 [8, 2048, 1024], P('sp', None, 'tp')
- gradient_down: float32 [8, 1024, 2048], P('sp', 'tp')
The draws below stay inside these ranges and needn't reach their ends.
Inputs may be any that keep to these rules, and one draw needn't show every extreme that they name: `expert_ids`: the two experts of a token differ. Among the rows of one index of sp, at most 60 routes name the same expert, and in every draw some expert is named by exactly 60 of them.
All inputs are finite; a program needn't handle non-finite values.
Results may differ from the reference program's by a relative error of at most 0.012.
Values may be sent and summed in bfloat16 or wider, within the bound.
A program may use at most 64 MiB of HBM per device.

```python
import math
import jax
import jax.numpy as jnp
import numpy as np
from jax import lax

D = 2048
C = 1024
F = 1024
K = 31
TOK_DEV = 192
TOKENS = 1536
EXPERTS = 8
CAP = 60
N_SP = 8
N_TP = 4


def draw_filtered(key, part):
    keys = jax.random.split(jax.random.fold_in(key, 17), 3)
    jitter = jax.random.uniform(keys[0], (C,), jnp.float32, 0.0, 1.0)
    channel_scale = jnp.exp(jnp.log(10.0) * (jnp.arange(C, dtype=jnp.float32) + jitter * C / 4.0) / (1.25 * C))
    row_scale = jnp.exp(jax.random.uniform(keys[1], (TOKENS, 1), jnp.float32, 0.0, jnp.log(10.0)))
    values = jax.random.normal(keys[2], (TOKENS, C), jnp.float32) * channel_scale * row_scale
    return jnp.clip(values, -1000.0, 1000.0).astype(jnp.bfloat16)


def strengthened(array, stream_key, source, target, parts, factor):
    owner, partner = [(jnp.arange(array.shape[dim]) // (array.shape[dim] // parts)).reshape([-1 if axis == dim else 1 for axis in range(array.ndim)]) for dim in (source, target)]
    chosen = jax.random.permutation(stream_key, parts)[partner]
    strong = (owner == chosen) | (owner == (partner + parts // 2) % parts)
    return jnp.where(strong, factor * array, array)


def level_of(key, shape, cuts, low, top_value):
    gain, own = 1.0, jax.random.fold_in(key, 6)
    for axis_at, blocks in cuts:
        draws = jnp.exp(jax.random.uniform(jax.random.fold_in(own, axis_at), (blocks,), jnp.float32, low / len(cuts), top_value / len(cuts)))
        gain = gain * jnp.repeat(draws, shape[axis_at] // blocks).reshape([-1 if axis == axis_at else 1 for axis in range(len(shape))])
    return gain


def shared_out(own_key, own, number, rows, number_of, top, limit, slope):
    ranking = jax.random.permutation(own_key, number_of)
    heavy_load, ordinary = load_shares(number_of, rows * top, limit, slope, True), load_shares(number_of, rows * top, limit, slope, False)
    places = jnp.arange(number_of)

    def named(sizes, offset_by):
        used = int((sizes > 0).sum())
        fixed = max(1, used // 4)
        shifted = fixed + (places - fixed + offset_by * (used - fixed)) % max(1, number_of - fixed)
        return jnp.zeros((number_of,), jnp.int32).at[ranking[jnp.where(places < fixed, places, shifted)]].set(jnp.asarray(sizes, jnp.int32))

    sizes = jnp.where(number % 4 == 0, named(heavy_load, number // 4), named(ordinary, number - number // 4 - 1))
    mixed = jax.random.permutation(jax.random.fold_in(own, 3), number_of)
    giver, sink = mixed[0:number_of // 2 * 2:2], mixed[1:number_of // 2 * 2:2]
    room = jnp.minimum(sizes[giver] - 1, limit - sizes[sink]) // 2
    room = jnp.where((giver == ranking[0]) | (sink == ranking[0]) | (sizes[sink] == 0), 0, jnp.maximum(room, 0))
    shifted = jax.random.randint(jax.random.fold_in(own, 4), (number_of // 2,), 0, 1 << 20) % (room + 1)
    sizes = sizes.at[giver].add(-shifted).at[sink].add(shifted)
    items = jnp.searchsorted(jnp.cumsum(sizes), jnp.arange(rows * top), side="right").astype(jnp.int32)
    listing = items.reshape(top, rows).T
    listing = listing[jax.random.permutation(jax.random.fold_in(own, 1), rows)]
    offset_by = jax.random.randint(jax.random.fold_in(own, 2), (rows, 1), 0, top)
    return jnp.take_along_axis(listing, (jnp.arange(top)[None, :] + offset_by) % top, axis=1)


def load_shares(amount, total, reach, skew, full):
    weights = [(1 << 20) // math.isqrt(grade ** skew) + 1 for grade in range(1, amount + 1)]
    largest = reach if full else min(reach, max(-(-total // amount), total * weights[0] // sum(weights)))
    least = 1 if total - largest >= amount - 1 else 0
    holding, spare = [largest] + [least] * (amount - 1), total - largest - least * (amount - 1)
    while spare > 0:
        free = [i for i in range(1, amount) if holding[i] < largest] or [i for i in range(1, amount) if holding[i] < reach]
        mass, left = sum([weights[i] for i in free]), spare
        for i in free:
            addition = min(reach - holding[i], max(1, left * weights[i] // mass), spare)
            holding[i] = holding[i] + addition
            spare = spare - addition
    return np.array(holding)


def noise(rng, shape, width, limit, cuts=(), held_as=jnp.bfloat16):
    values = width * jax.random.normal(rng, shape, jnp.float32)
    if cuts:
        values = values * level_of(rng, shape, cuts, -0.22, 0.18)
    return jnp.clip(values, -limit, limit).astype(held_as)


def gaussian_with(stream_key, shape, deviation, bound, shards, heavy, kind=jnp.bfloat16):
    array = deviation * jax.random.normal(stream_key, shape, jnp.float32)
    if shards:
        array = array * level_of(stream_key, shape, shards, -0.22, 0.18)
    return jnp.clip(strengthened(array, jax.random.fold_in(stream_key, 3), *heavy), -bound, bound).astype(kind)


def setup_inputs(seed: int = 0) -> dict:
    key_of = jax.random.split(jax.random.key(seed), 16)
    stream = noise(key_of[0], (TOKENS, D), 1.0, 6.0, ((0, 8),))
    upstream = gaussian_with(key_of[1], (TOKENS, D), 1.0, 6.0, ((0, 8),), (0, 1, 8, 2.0))
    expert_gain = jnp.clip(1.0 + 0.18 * jax.random.normal(key_of[2], (D,), jnp.float32), 0.1, 1.9)
    expert_ids_keys = jax.random.split(jax.random.fold_in(key_of[3], 1), TOKENS // TOK_DEV)
    expert_ids_turns = jax.random.permutation(jax.random.fold_in(key_of[3], 3), TOKENS // TOK_DEV)
    expert_ids = jax.vmap(lambda own, number: shared_out(jax.random.fold_in(key_of[3], 2), own, number, TOK_DEV, EXPERTS, 2, CAP, 1))(expert_ids_keys, expert_ids_turns).reshape((TOKENS, 2))
    group_weight = jnp.clip(0.25 + 0.75 * jax.random.uniform(key_of[4], (TOKENS,), jnp.float32) ** level_of(key_of[4], (TOKENS,), ((0, 8),), -0.2, 0.2), 0.25, 1.0)
    pair_scores = noise(key_of[5], (TOKENS, 2), 1.5, 6.0, ((0, 8),), jnp.float32)
    gate_weight = noise(key_of[6], (EXPERTS, D, F), D ** -0.5, 0.125, ((0, 8), (2, 4)))
    up_weight = noise(key_of[7], (EXPERTS, D, F), D ** -0.5, 0.125, ((0, 8), (2, 4)))
    down_weight = noise(key_of[8], (EXPERTS, F, D), F ** -0.5, 0.1875, ((0, 8), (1, 4)))
    mixer_weight = noise(key_of[9], (C, D), C ** -0.5, 0.1875, ((0, 4),))
    filtered = draw_filtered(jax.random.fold_in(key_of[15], 71), 0)
    channel_gain = jnp.clip(1.0 + 0.18 * jax.random.normal(key_of[11], (C,), jnp.float32), 0.1, 1.9)
    kernel_taps = noise(key_of[12], (K, C), K ** -0.5, 1.0, ((1, 4),), jnp.float32)
    value_branch = noise(key_of[13], (TOKENS, C), 1.0, 6.0, ((0, 8), (1, 4)))
    gate_branch = noise(key_of[14], (TOKENS, C), 1.5, 6.0, ((0, 8), (1, 4)))
    return dict(stream=stream, upstream=upstream, expert_gain=expert_gain, expert_ids=expert_ids, group_weight=group_weight, pair_scores=pair_scores, gate_weight=gate_weight, up_weight=up_weight, down_weight=down_weight, mixer_weight=mixer_weight, filtered=filtered, channel_gain=channel_gain, kernel_taps=kernel_taps, value_branch=value_branch, gate_branch=gate_branch)


EPS = 1e-06

def route_slots(routes, capacity, experts):
    flat = routes.reshape(-1)
    onehot = (flat[:, None] == jnp.arange(experts, dtype=jnp.int32)[None, :]).astype(jnp.int32)
    before = jnp.cumsum(onehot, axis=0) - onehot
    position = lax.optimization_barrier(jnp.sum(before * onehot, axis=1))
    slots = (flat * capacity + position).astype(jnp.int32)
    total = flat.shape[0]
    source = jnp.full((experts * capacity,), total, jnp.int32).at[slots].set(jnp.arange(total, dtype=jnp.int32))
    return (slots, source)

def silu_slope(value, sigma):
    return sigma * (1.0 + value * (1.0 - sigma))

def reference(stream, upstream, expert_gain, expert_ids, group_weight, pair_scores, gate_weight, up_weight, down_weight, mixer_weight, filtered, channel_gain, kernel_taps, value_branch, gate_branch):
    stream_f = stream.astype(jnp.float32)
    inv_rms = lax.rsqrt(lax.optimization_barrier(jnp.mean(stream_f * stream_f, axis=1, keepdims=True)) + EPS)
    normed = (stream_f * inv_rms * expert_gain).astype(jnp.bfloat16)
    spread = pair_scores[:, 0] - pair_scores[:, 1]
    route_weight = group_weight[:, None] * jnp.stack([jax.nn.sigmoid(spread), jax.nn.sigmoid(-spread)], axis=1)
    per_block = expert_ids.reshape(N_SP, TOK_DEV, 2)
    slots, source = jax.vmap(lambda routes: route_slots(routes, CAP, EXPERTS))(per_block)
    routes_dev = 2 * TOK_DEV
    offsets = (jnp.arange(N_SP, dtype=jnp.int32) * routes_dev)[:, None]
    global_source = jnp.where(source < routes_dev, source + offsets, 2 * TOKENS).astype(jnp.int32)
    table = global_source.reshape(N_SP, EXPERTS, CAP).transpose(1, 0, 2).reshape(EXPERTS, N_SP * CAP)
    normed_ext = jnp.concatenate([normed, jnp.zeros((1, D), jnp.bfloat16)], axis=0)
    upstream_ext = jnp.concatenate([upstream, jnp.zeros((1, D), jnp.bfloat16)], axis=0)
    weight_ext = jnp.concatenate([route_weight.reshape(-1), jnp.zeros((1,), jnp.float32)], axis=0)
    block = F // N_TP

    def one_expert(args):
        index, gate_w, up_w, down_w = args
        token_index = index // 2
        rows = normed_ext[token_index]
        cots = (weight_ext[index][:, None] * upstream_ext[token_index].astype(jnp.float32)).astype(jnp.bfloat16)
        pre_gate = jnp.dot(rows, gate_w, preferred_element_type=jnp.float32)
        pre_up = jnp.dot(rows, up_w, preferred_element_type=jnp.float32)
        sigma = jax.nn.sigmoid(pre_gate)
        silu_gate = pre_gate * sigma
        hidden = (silu_gate * pre_up).astype(jnp.bfloat16)
        grad_hidden = jnp.dot(cots, down_w.T, preferred_element_type=jnp.float32)
        grad_pre_gate = (grad_hidden * pre_up * silu_slope(pre_gate, sigma)).astype(jnp.bfloat16)
        grad_pre_up = (grad_hidden * silu_gate).astype(jnp.bfloat16)
        grad_gate_w = jnp.dot(rows.T, grad_pre_gate, preferred_element_type=jnp.float32)
        grad_up_w = jnp.dot(rows.T, grad_pre_up, preferred_element_type=jnp.float32)
        grad_down_w = jnp.dot(hidden.T, cots, preferred_element_type=jnp.float32)
        terms = jnp.einsum('rtf,dtf->trd', grad_pre_gate.reshape(-1, N_TP, block).astype(jnp.float32), gate_w.reshape(D, N_TP, block).astype(jnp.float32))
        terms = terms + jnp.einsum('rtf,dtf->trd', grad_pre_up.reshape(-1, N_TP, block).astype(jnp.float32), up_w.reshape(D, N_TP, block).astype(jnp.float32))
        rounded = lax.optimization_barrier(terms.astype(jnp.bfloat16))
        returned = lax.optimization_barrier(jnp.sum(rounded.astype(jnp.float32), axis=0)).astype(jnp.bfloat16)
        return (grad_gate_w, grad_up_w, grad_down_w, returned)
    gradient_gate, gradient_up, gradient_down, returned = lax.map(one_expert, (table, gate_weight, up_weight, down_weight))
    returned_flat = returned.reshape(EXPERTS * N_SP * CAP, D)
    expert_of = slots // CAP
    position = slots % CAP
    flat_index = (expert_of * (N_SP * CAP) + jnp.arange(N_SP, dtype=jnp.int32)[:, None] * CAP + position).astype(jnp.int32).reshape(TOKENS, 2)
    grad_normed = returned_flat[flat_index[:, 0]].astype(jnp.float32) + returned_flat[flat_index[:, 1]].astype(jnp.float32)
    weighted = grad_normed * expert_gain
    inner = lax.optimization_barrier(jnp.mean(weighted * stream_f, axis=1, keepdims=True))
    grad_stream = (upstream.astype(jnp.float32) + inv_rms * weighted - stream_f * inv_rms * inv_rms * inv_rms * inner).astype(jnp.bfloat16)
    grad_act = jnp.dot(grad_stream, mixer_weight.T, preferred_element_type=jnp.float32)
    filt = filtered.astype(jnp.float32)
    mean_c = lax.optimization_barrier(jnp.mean(filt, axis=1, keepdims=True))
    raw = filt - mean_c
    inv_std = lax.rsqrt(lax.optimization_barrier(jnp.mean(raw * raw, axis=1, keepdims=True)) + EPS)
    centred = raw * inv_std
    normal_out = centred * channel_gain
    sigma = jax.nn.sigmoid(normal_out)
    activated = (normal_out * sigma).astype(jnp.bfloat16)
    gradient_mixer = jnp.dot(grad_stream.T, activated, preferred_element_type=jnp.float32)
    grad_centred = grad_act * silu_slope(normal_out, sigma) * channel_gain
    first_mean = lax.optimization_barrier(jnp.mean(grad_centred, axis=1, keepdims=True))
    second_mean = lax.optimization_barrier(jnp.mean(grad_centred * centred, axis=1, keepdims=True))
    grad_filtered = (inv_std * (grad_centred - first_mean - centred * second_mean)).astype(jnp.bfloat16)
    extended = jnp.concatenate([grad_filtered.astype(jnp.float32), jnp.zeros((K - 1, C), jnp.float32)], axis=0)
    grad_mixed = lax.conv_general_dilated(extended[None], kernel_taps[::-1][:, None, :], (1,), 'VALID', dimension_numbers=('NWC', 'WIO', 'NWC'), feature_group_count=C, precision=lax.Precision.HIGHEST)[0]
    sig_gate = jax.nn.sigmoid(gate_branch.astype(jnp.float32))
    gradient_value = (grad_mixed * sig_gate).astype(jnp.bfloat16)
    gradient_gating = (grad_mixed * value_branch.astype(jnp.float32) * sig_gate * (1.0 - sig_gate)).astype(jnp.bfloat16)
    return (gradient_value, gradient_gating, gradient_mixer, gradient_gate, gradient_up, gradient_down)
```

```python
import functools

import jax
import jax.numpy as jnp
from jax import lax
from jax.experimental import pallas as pl
from jax.experimental.pallas import tpu as pltpu
from jax.sharding import PartitionSpec as P

EPS = 1e-06
MESH = pl.DeviceIdType.MESH
F32 = jnp.float32
BF16 = jnp.bfloat16
HIGHEST = lax.Precision.HIGHEST
UNROLL = 8
DIRECT = 2


def silu_slope(value, sigma):
    return sigma * (1.0 + value * (1.0 - sigma))


def contract_last(left, right, precision=None):
    return lax.dot_general(
        left, right, (((1,), (1,)), ((), ())), preferred_element_type=F32, precision=precision
    )


def contract_first(left, right):
    return lax.dot_general(left, right, (((0,), (0,)), ((), ())), preferred_element_type=F32)


def dot(left, right):
    return jnp.dot(left, right, preferred_element_type=F32)


def round_up(value, unit):
    return -(-value // unit) * unit


def flip(index, mask):
    bit = 1
    while bit <= mask:
        if mask & bit:
            index = index + bit - 2 * bit * ((index // bit) % 2)
        bit *= 2
    return index


def either(index, mask, limit):
    if isinstance(mask, int):
        return flip(index, mask)
    bit, total = 1, 0
    while bit < limit:
        total = total + bit * (((index // bit) % 2 + (mask // bit) % 2) % 2)
        bit *= 2
    return total


def low_bit(mask):
    return mask & -mask


def bits_below(limit):
    found, bit = [], 1
    while bit < limit:
        found.append(bit)
        bit *= 2
    return found[::-1]


def remote(src, dst, send, recv, where):
    return pltpu.make_async_remote_copy(
        src_ref=src, dst_ref=dst, send_sem=send, recv_sem=recv, device_id=where, device_id_type=MESH
    )


def start_of(i, unit):
    return i * unit if isinstance(i, int) else pl.multiple_of(i * unit, unit)


class Spread:
    def __init__(self, axis, place, index, count, send, recv):
        self.axis, self.place, self.index, self.count = axis, place, index, count
        self.send_sem, self.recv_sem = send, recv

    def copy(self, mask, bit):
        ref = self.place(flip(self.index, mask))
        return remote(
            ref,
            ref,
            self.send_sem(mask | bit),
            self.recv_sem(mask | bit),
            {self.axis: flip(self.index, bit)},
        )

    def wait(self, mask):
        ref = self.place(flip(self.index, mask))
        where = {self.axis: flip(self.index, low_bit(mask))}
        remote(ref, ref, self.send_sem(mask), self.recv_sem(mask), where).wait_recv()

    def begin(self):
        for bit in bits_below(self.count):
            self.copy(0, bit).start()

    def masks(self):
        return sorted(range(1, self.count), key=lambda m: (bin(m).count("1"), -low_bit(m)))

    def relay(self):
        for mask in self.masks():
            onward = bits_below(low_bit(mask))
            if onward:
                self.wait(mask)
                for bit in onward:
                    self.copy(mask, bit).start()

    def arrived(self):
        for mask in self.masks():
            if not bits_below(low_bit(mask)):
                self.wait(mask)

    def sent(self):
        for mask in range(1, self.count):
            self.copy(mask - low_bit(mask), low_bit(mask)).wait_send()


class Direct:
    def __init__(self, place, index, count, send, recv):
        self.place, self.index, self.count = place, index, count
        self.send_sem, self.recv_sem = send, recv

    def copy(self, mask, origin):
        ref = self.place(origin)
        return remote(
            ref, ref, self.send_sem.at[mask], self.recv_sem.at[mask], {"tp": flip(self.index, mask)}
        )

    def begin(self):
        for mask in range(1, self.count):
            self.copy(mask, self.index).start()

    def arrived(self):
        for mask in range(1, self.count):
            self.copy(mask, flip(self.index, mask)).wait_recv()

    def sent(self):
        for mask in range(1, self.count):
            self.copy(mask, self.index).wait_send()


def bands_of(n):
    sizes = (n // 4, n // 4, n // 4, n // 8, n // 8)
    found, first = [], 0
    for size in sizes:
        found.append((first, first + size))
        first += size
    return found


def direct_of(n):
    return n // DIRECT


def each(first, last, step):
    if last - first <= UNROLL:
        for i in range(first, last):
            step(i)
        return

    def run(i, carry):
        step(i)
        return carry

    lax.fori_loop(first, last, run, 0)


INPUTS = (
    "ids",
    "weight",
    "scores",
    "gain",
    "stream",
    "upstream",
    "filtered",
    "gate_w",
    "up_w",
    "down_w",
    "channel_gain",
    "mixer",
    "taps",
    "value",
    "gate",
)
OUTPUTS = ("out_value", "out_gating", "out_mixer", "out_gate", "out_up", "out_down")


def layer_kernel(n, groups, pcap, names, *refs):
    r = dict(zip(names, refs))
    v = {name: r["v_" + name] for name in INPUTS}
    me, tp = lax.axis_index("sp"), lax.axis_index("tp")
    tokens, width = v["stream"].shape
    column = width // groups
    here = v["filtered"].shape[1]
    channels = here * groups
    slots = n * pcap
    portion = tokens // groups
    db = width // n
    pdb = r["grad_all"].shape[1]
    reach = v["taps"].shape[0] - 1
    hpad = r["halo_in"].shape[0]
    bands = bands_of(n)
    near = direct_of(n)
    top = n // 2
    half = groups // 2
    scope = jax.named_scope

    def peer(m):
        return either(me, m, n)

    barrier = pltpu.get_barrier_semaphore()
    each(
        1,
        n,
        lambda m: pl.semaphore_signal(
            barrier, inc=1, device_id={"sp": peer(m)}, device_id_type=MESH
        ),
    )
    for k in range(1, groups):
        pl.semaphore_signal(barrier, inc=1, device_id={"tp": flip(tp, k)}, device_id_type=MESH)
    before = lax.rem(me + n - 1, n)

    def load(name):
        return pltpu.make_async_copy(r[name], v[name], r["load"].at[INPUTS.index(name)])

    for name in INPUTS:
        load(name).start()

    with scope("slots"):
        earlier = (
            (
                lax.broadcasted_iota(jnp.int32, (tokens, tokens), 0)
                < lax.broadcasted_iota(jnp.int32, (tokens, tokens), 1)
            )
            .astype(F32)
            .astype(BF16)
        )
        eye = (
            lax.broadcasted_iota(jnp.int32, (tokens, tokens), 0)
            == lax.broadcasted_iota(jnp.int32, (tokens, tokens), 1)
        ).astype(F32)
        block_id = lax.broadcasted_iota(jnp.int32, (n, tokens), 0)
        expert = jnp.bitwise_xor(block_id, me)
        slot_at = lax.broadcasted_iota(jnp.int32, (slots, tokens), 0)
        load("ids").wait()
        hit_a = (expert == v["ids"][0:1]).astype(F32)
        hit_b = (expert == v["ids"][1:2]).astype(F32)
        ahead_a = dot(hit_a.astype(BF16), earlier)
        ahead_b = dot(hit_b.astype(BF16), earlier) + jnp.sum(hit_a, axis=1, keepdims=True)
        base = (block_id * pcap).astype(F32)
        slot_a = jnp.sum(hit_a * (ahead_a + base), axis=0, keepdims=True)
        slot_b = jnp.sum(hit_b * (ahead_b + base), axis=0, keepdims=True)
        first = (slot_at == slot_a.astype(jnp.int32)).astype(F32).astype(BF16)
        second = (slot_at == slot_b.astype(jnp.int32)).astype(F32).astype(BF16)
        both = first + second
        r["first"][...] = first
        r["second"][...] = second
        for name in ("weight", "scores", "gain"):
            load(name).wait()
        spread = v["scores"][0:1] - v["scores"][1:2]
        weight_a = v["weight"][...] * jax.nn.sigmoid(spread)
        weight_b = v["weight"][...] * jax.nn.sigmoid(-spread)
        line = lax.broadcasted_iota(jnp.int32, (8, tokens), 0)
        small = jnp.where(
            line == 0,
            weight_a,
            jnp.where(line == 1, weight_b, jnp.where(line == 2, slot_a, slot_b)),
        )
        small = contract_last(eye, small, HIGHEST)
        weight_a, weight_b = small[:, 0:1], small[:, 1:2]
        slot_col_a = small[:, 2:3].astype(jnp.int32)
        slot_col_b = small[:, 3:4].astype(jnp.int32)

    with scope("rows"):
        load("stream").wait()
        load("upstream").wait()
        inv_rms = jnp.zeros((tokens, 1), F32)
        for q in range(groups):
            piece = v["stream"][:, q * column : (q + 1) * column].astype(F32)
            inv_rms = inv_rms + jnp.sum(piece * piece, axis=1, keepdims=True)
        inv_rms = lax.rsqrt(inv_rms / width + EPS)

        def quarter(q):
            return pl.ds(start_of(q, column), column)

        def routed(cols, rows):
            normed = (v["stream"][:, cols].astype(F32) * inv_rms * v["gain"][:, cols]).astype(BF16)
            up = v["upstream"][:, cols].astype(F32)
            scaled_a = (weight_a * up).astype(BF16)
            scaled_b = (weight_b * up).astype(BF16)
            one, two = r["first"][rows], r["second"][rows]
            return (
                dot(one + two, normed).astype(BF16),
                (dot(one, scaled_a) + dot(two, scaled_b)).astype(BF16),
            )

        mine_q = quarter(tp)
        side = lax.rem(tp, 2)

        def lane_q(h):
            return quarter(side + 2 * h)

        def stage(cols, lo, hi, at, rows_to, cots_to):
            out_rows, out_cots = routed(cols, slice(lo * pcap, hi * pcap))
            rows_to[at] = out_rows
            cots_to[at] = out_cots

        for h in range(half):
            at = (slice(0, (near - 1) * pcap), slice(h * column, (h + 1) * column))
            stage(lane_q(h), 1, near, at, r["near_rows"], r["near_cots"])

    pairs = ((r["send_rows"], r["rows"]), (r["send_cots"], r["cots"]))
    close = (r["near_rows"], r["near_cots"])

    def block(m):
        return pl.ds(start_of(m, pcap), pcap)

    def near_copy(a, m, h):
        return remote(
            close[a].at[block(m - 1), pl.ds(h * column, column)],
            pairs[a][1].at[block(m), lane_q(h)],
            r["near_send"].at[a, m, h],
            r["near_recv"].at[a, m, h],
            {"sp": peer(m)},
        )

    def core_share(a, m, h):
        ref = pairs[a][1].at[block(m), lane_q(h)]
        return remote(
            ref, ref, r["share_send"].at[a, m, h], r["share_recv"].at[a, m, h], {"tp": flip(tp, 1)}
        )

    def sp_copy(a, m):
        src, full = pairs[a]
        return remote(
            src.at[block(m - near)],
            full.at[block(m), mine_q],
            r["sp_send"].at[a, m],
            r["sp_recv"].at[a, m],
            {"sp": peer(m)},
        )

    with scope("barrier"):
        pl.semaphore_wait(barrier, n - 1 + groups - 1)

    def send_near(m):
        for a in range(2):
            for h in range(half):
                near_copy(a, m, h).start()

    def send(m):
        for a in range(2):
            sp_copy(a, m).start()

    def send_any(lo, hi):
        each(lo, min(hi, near), send_near)
        each(max(lo, near), hi, send)

    parts = ((1, n // 4), (n // 2, 3 * n // 4), (n // 4, n // 2), (3 * n // 4, n))
    send_any(*parts[0])
    with scope("rows2"):
        stage(mine_q, near, n, slice(0, (n - near) * pcap), r["send_rows"], r["send_cots"])
    for lo, hi in parts[1:]:
        send_any(lo, hi)

    with scope("stats"):
        load("filtered").wait()
        filt = v["filtered"][...]
        square = filt.astype(F32) * filt.astype(F32)
        high = square.astype(BF16)
        low = (square - high.astype(F32)).astype(BF16)
        ones = jnp.ones((8, here), BF16)
        total = contract_last(ones, filt)
        total_square = contract_last(ones, high) + contract_last(ones, low)
        r["stats"][tp] = jnp.where(line == 0, total, total_square)
        sums = Direct(lambda o: r["stats"].at[o], tp, groups, r["st_send"], r["st_recv"])
        sums.begin()

    with scope("own"):
        for q in range(groups):
            cols = slice(q * column, (q + 1) * column)
            own_rows, own_cots = routed(cols, slice(0, pcap))
            r["rows"][0:pcap, cols] = own_rows
            r["cots"][0:pcap, cols] = own_cots
        lane = lax.broadcasted_iota(jnp.int32, (tokens, slots), 1)
        r["places"][...] = (
            ((lane == slot_col_a) | (lane == slot_col_b)).astype(F32).astype(BF16)
        )

    def gather(a, m):
        return Spread(
            "tp",
            lambda o: pairs[a][1].at[block(m), quarter(o)],
            tp,
            groups,
            lambda k: r["tp_send"].at[a, m, k],
            lambda k: r["tp_recv"].at[a, m, k],
        )

    def arrive_near(m):
        for a in range(2):
            for h in range(half):
                near_copy(a, m, h).wait_recv()
                core_share(a, m, h).start()

    def arrived_near(m):
        for a in range(2):
            for h in range(half):
                core_share(a, m, h).wait_recv()

    def arrive(m):
        for a in range(2):
            sp_copy(a, m).wait_recv()
            gather(a, m).begin()

    def relay(m):
        for a in range(2):
            gather(a, m).relay()

    def arrived(m):
        for a in range(2):
            gather(a, m).arrived()

    def band(c):
        return pl.ds(bands[c][0] * pcap, (bands[c][1] - bands[c][0]) * pcap)

    wide = 2 * v["gate_w"].shape[1]
    turned = wide // 2

    def turn():
        tile = min(256, width)
        for t in range(0, width, tile):
            at = slice(t, t + tile)
            for k, name in enumerate(("gate_w", "up_w")):
                r["back_w"][k * turned : (k + 1) * turned, at] = v[name][at].T
            r["down_t"][at] = v["down_w"][:, at].T

    def compute(c):
        at = band(c)
        rows, cots = r["rows"][at], r["cots"][at]
        pre_gate = dot(rows, v["gate_w"][...])
        pre_up = dot(rows, v["up_w"][...])
        grad_hidden = dot(cots, r["down_t"][...])
        sigma = jax.nn.sigmoid(pre_gate)
        silu_gate = pre_gate * sigma
        grad_pre_gate = (grad_hidden * pre_up * silu_slope(pre_gate, sigma)).astype(BF16)
        grad_pre_up = (grad_hidden * silu_gate).astype(BF16)
        r["hidden"][at] = (silu_gate * pre_up).astype(BF16)
        r["gpg"][at] = grad_pre_gate
        r["gpu"][at] = grad_pre_up
        slopes_in = jnp.concatenate([grad_pre_gate, grad_pre_up], axis=1)
        for q in range(groups):
            cols = slice(q * column, (q + 1) * column)
            r["partial"][at, cols] = dot(slopes_in, r["back_w"][:, cols]).astype(BF16)

    mate = flip(tp, 1)
    mine = tp // 2

    def core_copy(c, h):
        return remote(
            r["partial"].at[band(c), quarter(lax.rem(mate, 2) + 2 * h)],
            r["halves"].at[band(c), pl.ds(h * column, column)],
            r["core_send"].at[c, h],
            r["core_recv"].at[c, h],
            {"tp": mate},
        )

    def cross(c, k):
        return remote(
            r["passing"].at[band(c), quarter(flip(mine, k))],
            r["crossed"].at[band(c), pl.ds((k - 1) * column, column)],
            r["x_send"].at[c, k],
            r["x_recv"].at[c, k],
            {"tp": flip(tp, 2 * k)},
        )

    def start_core(c):
        for h in range(half):
            core_copy(c, h).start()

    def add_core(c):
        for h in range(half):
            core_copy(c, h).wait_recv()
        for h in range(half):
            cols = pl.ds(h * column, column)
            own = r["partial"][band(c), quarter(lax.rem(tp, 2) + 2 * h)].astype(F32)
            r["passing"][band(c), cols] = (
                own + r["halves"][band(c), cols].astype(F32)
            ).astype(BF16)
        for k in range(1, half):
            cross(c, k).start()

    def home_copy(m):
        return remote(
            r["outgoing"].at[block(m)],
            r["back"].at[block(m)],
            r["home_send"].at[m],
            r["home_recv"].at[m],
            {"sp": peer(m)},
        )

    def add_cross(c):
        for k in range(1, half):
            cross(c, k).wait_recv()
        total = r["passing"][band(c), quarter(mine)].astype(F32)
        for k in range(1, half):
            total = total + r["crossed"][band(c), pl.ds((k - 1) * column, column)].astype(F32)
        r["outgoing"][band(c)] = total.astype(BF16)
        each(max(1, bands[c][0]), bands[c][1], lambda m: home_copy(m).start())

    def act_rows(s):
        return pl.ds(start_of(s, tokens), tokens)

    acts = Spread(
        "sp",
        lambda o: r["act_all"].at[act_rows(o)],
        me,
        n,
        lambda m: r["act_send"].at[m],
        lambda m: r["act_recv"].at[m],
    )

    def early(bit):
        acts.copy(0, bit).start()

    def arrivals(lo, hi):
        with scope("arrive#m=%d" % lo):
            each(lo, min(hi, near), arrive_near)

            def step(m):
                arrive(m)
                if isinstance(m, int):
                    if m > max(lo, near):
                        relay(m - 1)
                else:
                    pl.when(m > max(lo, near))(lambda: relay(m - 1))

            each(max(lo, near), hi, step)

    def lastrelay(hi):
        if hi > near:
            with scope("relay#m=%d" % (hi - 1)):
                relay(hi - 1)

    def whole(c):
        lo, hi = bands[c]
        with scope("finish#c=%d" % c):
            each(max(1, lo), min(hi, near), arrived_near)
            each(max(1, lo, near), hi, arrived)
        with scope("compute#c=%d" % c):
            compute(c)
            start_core(c)

    with scope("turn"):
        for name in ("gate_w", "up_w", "down_w"):
            load(name).wait()
        turn()
    with scope("normact"):
        sums.arrived()
        moments = r["stats"][0]
        for o in range(1, groups):
            moments = moments + r["stats"][o]
        moments = contract_last(eye, moments, HIGHEST)
        mean_c = moments[:, 0:1] / channels
        variance = moments[:, 1:2] / channels - mean_c * mean_c
        inv_std = lax.rsqrt(variance + EPS)
        load("channel_gain").wait()

        def norms():
            centred = (v["filtered"][...].astype(F32) - mean_c) * inv_std
            normal_out = centred * v["channel_gain"][...]
            return centred, normal_out, jax.nn.sigmoid(normal_out)

        _, normal_out, sig_norm = norms()
        r["act_all"][act_rows(me)] = (normal_out * sig_norm).astype(BF16)

    def addcore(c):
        with scope("addcore#c=%d" % c):
            add_core(c)

    def addcross(c):
        with scope("addcross#c=%d" % c):
            add_cross(c)

    def act_relay(masks):
        for mask in masks:
            onward = bits_below(low_bit(mask))
            if onward:
                acts.wait(mask)
                for bit in onward:
                    acts.copy(mask, bit).start()

    act_masks = acts.masks()
    quarter_n, last = n // 4, len(bands) - 1
    one, two, three = bands[1][0], bands[2][0], bands[3][0]
    final = bands[4][0]
    arrivals(1, one)
    lastrelay(one)
    whole(0)
    arrivals(two, three)
    addcore(0)
    lastrelay(three)
    whole(2)
    addcross(0)
    arrivals(one, two)
    addcore(2)
    lastrelay(two)
    whole(1)
    arrivals(three, final)
    addcore(1)
    addcross(2)
    arrivals(final, n)
    lastrelay(final)
    whole(3)
    for bit in bits_below(n):
        early(bit)
    lastrelay(n)
    addcross(1)
    addcore(3)
    whole(4)
    addcross(3)
    addcore(4)

    tile = min(256, width)

    def wgrad(left, pick):
        def step(t):
            cols = pl.ds(start_of(t, tile), tile)
            r[pick][cols] = contract_first(r["rows"][:, cols], r[left][...])

        lax.fori_loop(0, width // tile, lambda t, c: (step(t), c)[1], 0)

    def wgrad_down():
        def step(t):
            cols = pl.ds(start_of(t, tile), tile)
            r["out_down"][:, cols] = contract_first(r["hidden"][...], r["cots"][:, cols])

        lax.fori_loop(0, width // tile, lambda t, c: (step(t), c)[1], 0)

    with scope("wgrad_gate"):
        wgrad("gpg", "out_gate")
    with scope("addcross#c=%d" % last):
        add_cross(last)
        r["back"][0:pcap] = r["outgoing"][0:pcap]
    with scope("wgrad_up"):
        wgrad("gpu", "out_up")
    with scope("home"):
        each(1, n, lambda m: home_copy(m).wait_recv())
    with scope("combine"):
        r["grad_normed"][:, mine_q] = dot(r["places"][...], r["back"][...]).astype(BF16)
        normal = Spread(
            "tp",
            lambda o: r["grad_normed"].at[:, quarter(o)],
            tp,
            groups,
            lambda m: r["gn_send"].at[m],
            lambda m: r["gn_recv"].at[m],
        )
        normal.begin()
    with scope("actrelay2"):
        act_relay([m for m in act_masks if m <= top])
    with scope("wgrad_down"):
        wgrad_down()
    with scope("actrelay3"):
        act_relay([m for m in act_masks if m > top])
    with scope("gather"):
        normal.relay()
        normal.arrived()

    with scope("gradstream"):
        inner = jnp.zeros((tokens, 1), F32)
        for q in range(groups):
            at = slice(q * column, (q + 1) * column)
            weighted = r["grad_normed"][:, at].astype(F32) * v["gain"][:, at]
            inner = inner + jnp.sum(
                weighted * v["stream"][:, at].astype(F32), axis=1, keepdims=True
            )
        inner = inv_rms * inv_rms * inv_rms * (inner / width)
        for q in range(groups):
            at = slice(q * column, (q + 1) * column)
            weighted = r["grad_normed"][:, at].astype(F32) * v["gain"][:, at]
            r["grad_stream"][:, at] = (
                v["upstream"][:, at].astype(F32)
                + inv_rms * weighted
                - v["stream"][:, at].astype(F32) * inner
            ).astype(BF16)

    def part(s, o):
        start = pl.multiple_of(s * tokens + o * portion, portion)
        return r["grad_all"].at[pl.ds(start, portion)]

    my_rows = pl.ds(pl.multiple_of(tp * portion, portion), portion)
    if db == pdb:

        def cut(j):
            return r["grad_stream"].at[my_rows, pl.ds(pl.multiple_of(j * db, db), db)]

        r["grad_all"][act_rows(me)] = r["grad_stream"][
            :, pl.ds(pl.multiple_of(me * db, db), db)
        ]
    else:

        def pick(j):
            where = lax.broadcasted_iota(jnp.int32, (width, pdb), 0)
            lane = lax.broadcasted_iota(jnp.int32, (width, pdb), 1)
            return ((where == lane + j * db) & (lane < db)).astype(F32).astype(BF16)

        def stage(j):
            r["staged"][j] = dot(r["grad_stream"][my_rows], pick(j)).astype(BF16)

        each(0, n, stage)

        def cut(j):
            return r["staged"].at[j]

        r["grad_all"][act_rows(me)] = dot(r["grad_stream"][...], pick(me)).astype(BF16)

    def cut_copy(m, j, s):
        return remote(cut(j), part(s, tp), r["gs_send"].at[m], r["gs_recv"].at[m], {"sp": j})

    def spread_cut(m):
        s = peer(m)
        return Spread(
            "tp",
            lambda o: part(s, o),
            tp,
            groups,
            lambda k: r["ga_send"].at[m, k],
            lambda k: r["ga_recv"].at[m, k],
        )

    def cut_arrives(m):
        cut_copy(m, peer(m), peer(m)).wait_recv()
        spread_cut(m).begin()

    with scope("cutstart"):
        each(1, n, lambda m: cut_copy(m, peer(m), me).start())

    with scope("slopes"):
        load("mixer").wait()
        grad_act = contract_last(r["grad_stream"][...], v["mixer"][...])
        centred, normal_out, sig_norm = norms()
        grad_centred = grad_act * silu_slope(normal_out, sig_norm) * v["channel_gain"][...]
        ones = jnp.ones((8, here), F32)
        slope_sum = contract_last(ones, grad_centred, HIGHEST)
        slope_cross = contract_last(ones, grad_centred * centred, HIGHEST)
        r["slopes"][tp] = jnp.where(line == 0, slope_sum, slope_cross)
        meet = Direct(lambda o: r["slopes"].at[o], tp, groups, r["sl_send"], r["sl_recv"])
        meet.begin()
    with scope("cutarrive1"):
        each(1, top, cut_arrives)
    with scope("meet"):
        meet.arrived()
    with scope("gradfiltered"):
        sums_b = r["slopes"][0]
        for o in range(1, groups):
            sums_b = sums_b + r["slopes"][o]
        sums_b = contract_last(eye, sums_b, HIGHEST)
        grad_filtered = (
            inv_std
            * (grad_centred - sums_b[:, 0:1] / channels - centred * (sums_b[:, 1:2] / channels))
        ).astype(BF16)
        r["halo_out"][...] = grad_filtered[:hpad]
        r["ext"][:tokens] = grad_filtered.astype(F32)

        def halo_copy():
            return remote(
                r["halo_out"], r["halo_in"], r["halo_send"], r["halo_recv"], {"sp": before}
            )

        halo_copy().start()

    def conv(lo, hi):
        mixed = jnp.zeros((hi - lo, here), F32)
        for k in range(reach + 1):
            mixed = mixed + v["taps"][k : k + 1] * r["ext"][lo + reach - k : hi + reach - k]
        sig_gate = jax.nn.sigmoid(v["gate"][lo:hi].astype(F32))
        r["out_value"][lo:hi] = (mixed * sig_gate).astype(BF16)
        r["out_gating"][lo:hi] = (
            mixed * v["value"][lo:hi].astype(F32) * sig_gate * (1.0 - sig_gate)
        ).astype(BF16)

    with scope("cutarrive2"):
        each(top, n - n // 4, cut_arrives)
    with scope("conv1"):
        for name in ("taps", "value", "gate"):
            load(name).wait()
        conv(0, tokens - hpad)
    with scope("cutarrive3"):
        each(n - n // 4, n, cut_arrives)
    with scope("halo"):
        halo_copy().wait_recv()
        inside = jnp.where(me < n - 1, 1.0, 0.0)
        r["ext"][tokens:] = r["halo_in"][...].astype(F32) * inside
    with scope("conv2"):
        conv(tokens - hpad, tokens)
    with scope("cutrelay"):
        each(1, n, lambda m: spread_cut(m).relay())
    with scope("cutwait"):
        each(1, n, lambda m: spread_cut(m).arrived())
    with scope("actwait"):
        acts.arrived()
    with scope("mixer"):
        r["out_mixer"][...] = contract_first(r["grad_all"][...], r["act_all"][...])[:db]

    with scope("drain"):

        def sent(m):
            home_copy(m).wait_send()
            cut_copy(m, peer(m), me).wait_send()
            spread_cut(m).sent()

        def sent_near(m):
            for a in range(2):
                for h in range(half):
                    near_copy(a, m, h).wait_send()
                    core_share(a, m, h).wait_send()

        def sent_far(m):
            for a in range(2):
                sp_copy(a, m).wait_send()
                gather(a, m).sent()

        each(1, near, sent_near)
        each(near, n, sent_far)
        each(1, n, sent)
        sums.sent()
        normal.sent()
        meet.sent()
        acts.sent()
        halo_copy().wait_send()
        for c in range(len(bands)):
            for h in range(half):
                core_copy(c, h).wait_send()
            for k in range(1, half):
                cross(c, k).wait_send()


def flush_kernel(*refs):
    count = len(refs) // 2
    sems = refs[-1]
    copies = [
        pltpu.make_async_copy(refs[i], refs[count + i], sems.at[i]) for i in range(count)
    ]
    for copy in copies:
        copy.start()
    for copy in copies:
        copy.wait()


def body(
    stream,
    upstream,
    expert_gain,
    expert_ids,
    group_weight,
    pair_scores,
    gate_weight,
    up_weight,
    down_weight,
    mixer_weight,
    filtered,
    channel_gain,
    kernel_taps,
    value_branch,
    gate_branch,
):
    n, groups = lax.axis_size("sp"), lax.axis_size("tp")
    tokens, width = stream.shape
    capacity = max(2, 5 * tokens // (2 * n))
    pcap = round_up(capacity, 16)
    column = width // groups
    here = filtered.shape[1]
    hidden = gate_weight.shape[2]
    slots = n * pcap
    half = groups // 2
    db = width // n
    pdb = round_up(db, 128)
    hpad = round_up(kernel_taps.shape[0] - 1, 16)
    staged = (n, tokens // groups, pdb) if pdb != db else (1, 16, 128)
    chunks = len(bands_of(n))
    near = direct_of(n)
    dma = pltpu.SemaphoreType.DMA
    shape = jax.ShapeDtypeStruct
    inputs = dict(
        ids=expert_ids.T,
        weight=group_weight[None],
        scores=pair_scores.T,
        gain=expert_gain[None],
        stream=stream,
        upstream=upstream,
        filtered=filtered,
        gate_w=gate_weight[0],
        up_w=up_weight[0],
        down_w=down_weight[0],
        channel_gain=channel_gain[None],
        mixer=mixer_weight,
        taps=kernel_taps,
        value=value_branch,
        gate=gate_branch,
    )
    outs = dict(
        out_value=shape((tokens, here), BF16),
        out_gating=shape((tokens, here), BF16),
        out_mixer=shape((db, here), F32),
        out_gate=shape((width, hidden), F32),
        out_up=shape((width, hidden), F32),
        out_down=shape((hidden, width), F32),
    )
    scratch = {"v_" + name: pltpu.VMEM(inputs[name].shape, inputs[name].dtype) for name in INPUTS}
    scratch |= dict(
        first=pltpu.VMEM((slots, tokens), BF16),
        second=pltpu.VMEM((slots, tokens), BF16),
        places=pltpu.VMEM((tokens, slots), BF16),
        send_rows=pltpu.VMEM((slots - near * pcap, column), BF16),
        send_cots=pltpu.VMEM((slots - near * pcap, column), BF16),
        near_rows=pltpu.VMEM(((near - 1) * pcap, half * column), BF16),
        near_cots=pltpu.VMEM(((near - 1) * pcap, half * column), BF16),
        rows=pltpu.VMEM((slots, width), BF16),
        cots=pltpu.VMEM((slots, width), BF16),
        hidden=pltpu.VMEM((slots, hidden), BF16),
        back_w=pltpu.VMEM((2 * hidden, width), BF16),
        down_t=pltpu.VMEM((width, hidden), BF16),
        gpg=pltpu.VMEM((slots, hidden), BF16),
        gpu=pltpu.VMEM((slots, hidden), BF16),
        partial=pltpu.VMEM((slots, width), BF16),
        halves=pltpu.VMEM((slots, half * column), BF16),
        passing=pltpu.VMEM((slots, half * column), BF16),
        crossed=pltpu.VMEM((slots, max(1, half - 1) * column), BF16),
        outgoing=pltpu.VMEM((slots, column), BF16),
        back=pltpu.VMEM((slots, column), BF16),
        grad_normed=pltpu.VMEM((tokens, width), BF16),
        grad_stream=pltpu.VMEM((tokens, width), BF16),
        staged=pltpu.VMEM(staged, BF16),
        grad_all=pltpu.VMEM((n * tokens, pdb), BF16),
        act_all=pltpu.VMEM((n * tokens, here), BF16),
        stats=pltpu.VMEM((groups, 8, tokens), F32),
        slopes=pltpu.VMEM((groups, 8, tokens), F32),
        halo_out=pltpu.VMEM((hpad, here), BF16),
        halo_in=pltpu.VMEM((hpad, here), BF16),
        ext=pltpu.VMEM((tokens + hpad, here), F32),
        load=dma((len(INPUTS),)),
    )
    for name, dims in dict(
        sp=(2, n),
        near=(2, near, half),
        share=(2, near, half),
        tp=(2, n, groups),
        st=(groups,),
        core=(chunks, half),
        x=(chunks, half),
        home=(n,),
        gn=(groups,),
        act=(n,),
        gs=(n,),
        ga=(n, groups),
        sl=(groups,),
        halo=(),
    ).items():
        scratch[name + "_send"] = dma(dims)
        scratch[name + "_recv"] = dma(dims)
    names = (*INPUTS, *OUTPUTS, *scratch)
    vmem, hbm = pltpu.VMEM, pltpu.HBM
    results = pl.pallas_call(
        functools.partial(layer_kernel, n, groups, pcap, names),
        out_shape=[pltpu.VMEM(outs[name].shape, outs[name].dtype) for name in OUTPUTS],
        in_specs=[pl.BlockSpec(memory_space=hbm)] * len(INPUTS),
        out_specs=[pl.BlockSpec(memory_space=vmem)] * len(OUTPUTS),
        scratch_shapes=list(scratch.values()),
        compiler_params=pltpu.CompilerParams(
            collective_id=0, has_side_effects=True, vmem_limit_bytes=54 << 20
        ),
    )(*(inputs[name] for name in INPUTS))
    results = pl.pallas_call(
        flush_kernel,
        out_shape=[outs[name] for name in OUTPUTS],
        in_specs=[pl.BlockSpec(memory_space=vmem)] * len(OUTPUTS),
        out_specs=[pl.BlockSpec(memory_space=hbm)] * len(OUTPUTS),
        scratch_shapes=[dma((len(OUTPUTS),))],
        compiler_params=pltpu.CompilerParams(vmem_limit_bytes=1 << 20),
    )(*results)
    value, gating, mixer, gate, up, down = results
    return value, gating, mixer, gate[None], up[None], down[None]


def solution(mesh):
    return jax.shard_map(
        body,
        mesh=mesh,
        in_specs=(
            P("sp", None),
            P("sp", None),
            P(),
            P("sp", None),
            P("sp"),
            P("sp", None),
            P("sp", None, "tp"),
            P("sp", None, "tp"),
            P("sp", "tp", None),
            P("tp", None),
            P("sp", "tp"),
            P("tp"),
            P(None, "tp"),
            P("sp", "tp"),
            P("sp", "tp"),
        ),
        out_specs=(
            P("sp", "tp"),
            P("sp", "tp"),
            P("sp", "tp"),
            P("sp", None, "tp"),
            P("sp", None, "tp"),
            P("sp", "tp", None),
        ),
        check_vma=False,
    )
```

```python
import functools

import jax
import jax.numpy as jnp
from jax import lax
from jax.experimental import pallas as pl
from jax.experimental.pallas import tpu as pltpu
from jax.sharding import PartitionSpec as P

EPS = 1e-06
MESH = pl.DeviceIdType.MESH
F32 = jnp.float32
BF16 = jnp.bfloat16
HIGHEST = lax.Precision.HIGHEST
UNROLL = 8
DIRECT = 2


def silu_slope(value, sigma):
    return sigma * (1.0 + value * (1.0 - sigma))


def contract_last(left, right, precision=None):
    return lax.dot_general(
        left, right, (((1,), (1,)), ((), ())), preferred_element_type=F32, precision=precision
    )


def contract_first(left, right):
    return lax.dot_general(left, right, (((0,), (0,)), ((), ())), preferred_element_type=F32)


def dot(left, right):
    return jnp.dot(left, right, preferred_element_type=F32)


def round_up(value, unit):
    return -(-value // unit) * unit


def flip(index, mask):
    bit = 1
    while bit <= mask:
        if mask & bit:
            index = index + bit - 2 * bit * ((index // bit) % 2)
        bit *= 2
    return index


def either(index, mask, limit):
    if isinstance(mask, int):
        return flip(index, mask)
    bit, total = 1, 0
    while bit < limit:
        total = total + bit * (((index // bit) % 2 + (mask // bit) % 2) % 2)
        bit *= 2
    return total


def low_bit(mask):
    return mask & -mask


def bits_below(limit):
    found, bit = [], 1
    while bit < limit:
        found.append(bit)
        bit *= 2
    return found[::-1]


def remote(src, dst, send, recv, where):
    return pltpu.make_async_remote_copy(
        src_ref=src, dst_ref=dst, send_sem=send, recv_sem=recv, device_id=where, device_id_type=MESH
    )


def start_of(i, unit):
    return i * unit if isinstance(i, int) else pl.multiple_of(i * unit, unit)


class Spread:
    def __init__(self, axis, place, index, count, send, recv, last):
        self.axis, self.place, self.index, self.count = axis, place, index, count
        self.send_sem, self.recv, self.last = send, recv, last

    def recv_sem(self, mask):
        return self.last if mask % 2 else self.recv(mask // 2 - 1)

    def copy(self, mask, bit):
        ref = self.place(flip(self.index, mask))
        return remote(
            ref, ref, self.send_sem, self.recv_sem(mask | bit), {self.axis: flip(self.index, bit)}
        )

    def wait(self, mask):
        ref = self.place(flip(self.index, mask))
        where = {self.axis: flip(self.index, low_bit(mask))}
        remote(ref, ref, self.send_sem, self.recv_sem(mask), where).wait_recv()

    def begin(self):
        for bit in bits_below(self.count):
            self.copy(0, bit).start()

    def masks(self):
        return sorted(range(1, self.count), key=lambda m: (bin(m).count("1"), -low_bit(m)))

    def relay(self):
        for mask in self.masks():
            onward = bits_below(low_bit(mask))
            if onward:
                self.wait(mask)
                for bit in onward:
                    self.copy(mask, bit).start()

    def arrived(self, ref):
        where = {self.axis: flip(self.index, 1)}
        remote(ref, ref, self.send_sem, self.last, where).wait_recv()

    def sent(self, ref):
        where = {self.axis: flip(self.index, 1)}
        remote(ref, ref, self.send_sem, self.last, where).wait_send()


class Direct:
    def __init__(self, place, index, count, send, recv, others):
        self.place, self.index, self.count = place, index, count
        self.send_sem, self.recv_sem, self.others = send, recv, others

    def copy(self, ref, mask):
        return remote(ref, ref, self.send_sem, self.recv_sem, {"tp": flip(self.index, mask)})

    def begin(self):
        for mask in range(1, self.count):
            self.copy(self.place(self.index), mask).start()

    def arrived(self):
        self.copy(self.others, 1).wait_recv()

    def sent(self):
        self.copy(self.others, 1).wait_send()


def bands_of(n):
    sizes = (n // 4, n // 4, n // 8, n // 8, n // 8, n // 8)
    found, first = [], 0
    for size in sizes:
        found.append((first, first + size))
        first += size
    return found


def direct_of(n):
    return n // DIRECT


def each(first, last, step):
    if last - first <= UNROLL:
        for i in range(first, last):
            step(i)
        return

    def run(i, carry):
        step(i)
        return carry

    lax.fori_loop(first, last, run, 0)


INPUTS = (
    "ids",
    "weight",
    "scores",
    "gain",
    "stream",
    "upstream",
    "filtered",
    "gate_w",
    "up_w",
    "down_w",
    "channel_gain",
    "mixer",
    "taps",
    "value",
    "gate",
)
OUTPUTS = ("out_value", "out_gating", "out_mixer", "out_gate", "out_up", "out_down")


def layer_kernel(n, groups, pcap, names, *refs):
    r = dict(zip(names, refs))
    v = {name: r["v_" + name] for name in INPUTS}
    me, tp = lax.axis_index("sp"), lax.axis_index("tp")
    tokens, width = v["stream"].shape
    column = width // groups
    here = v["filtered"].shape[1]
    channels = here * groups
    slots = n * pcap
    portion = tokens // groups
    db = width // n
    pdb = r["grad_all"].shape[1]
    reach = v["taps"].shape[0] - 1
    hpad = r["halo_in"].shape[0]
    bands = bands_of(n)
    near = direct_of(n)
    top = n // 2
    half = groups // 2
    scope = jax.named_scope

    def peer(m):
        return either(me, m, n)

    barrier = pltpu.get_barrier_semaphore()
    each(
        1,
        n,
        lambda m: pl.semaphore_signal(
            barrier, inc=1, device_id={"sp": peer(m)}, device_id_type=MESH
        ),
    )
    for k in range(1, groups):
        pl.semaphore_signal(barrier, inc=1, device_id={"tp": flip(tp, k)}, device_id_type=MESH)
    before = lax.rem(me + n - 1, n)

    def load(name):
        return pltpu.make_async_copy(r[name], v[name], r["load"].at[INPUTS.index(name)])

    for name in INPUTS:
        load(name).start()

    with scope("slots"):
        earlier = (
            (
                lax.broadcasted_iota(jnp.int32, (tokens, tokens), 0)
                < lax.broadcasted_iota(jnp.int32, (tokens, tokens), 1)
            )
            .astype(F32)
            .astype(BF16)
        )
        eye = (
            lax.broadcasted_iota(jnp.int32, (tokens, tokens), 0)
            == lax.broadcasted_iota(jnp.int32, (tokens, tokens), 1)
        ).astype(F32)
        block_id = lax.broadcasted_iota(jnp.int32, (n, tokens), 0)
        expert = jnp.bitwise_xor(block_id, me)
        slot_at = lax.broadcasted_iota(jnp.int32, (slots, tokens), 0)
        load("ids").wait()
        hit_a = (expert == v["ids"][0:1]).astype(F32)
        hit_b = (expert == v["ids"][1:2]).astype(F32)
        ahead_a = dot(hit_a.astype(BF16), earlier)
        ahead_b = dot(hit_b.astype(BF16), earlier) + jnp.sum(hit_a, axis=1, keepdims=True)
        base = (block_id * pcap).astype(F32)
        slot_a = jnp.sum(hit_a * (ahead_a + base), axis=0, keepdims=True)
        slot_b = jnp.sum(hit_b * (ahead_b + base), axis=0, keepdims=True)
        first = (slot_at == slot_a.astype(jnp.int32)).astype(F32).astype(BF16)
        second = (slot_at == slot_b.astype(jnp.int32)).astype(F32).astype(BF16)
        both = first + second
        r["first"][...] = first
        r["second"][...] = second
        for name in ("weight", "scores", "gain"):
            load(name).wait()
        spread = v["scores"][0:1] - v["scores"][1:2]
        weight_a = v["weight"][...] * jax.nn.sigmoid(spread)
        weight_b = v["weight"][...] * jax.nn.sigmoid(-spread)
        line = lax.broadcasted_iota(jnp.int32, (8, tokens), 0)
        small = jnp.where(
            line == 0,
            weight_a,
            jnp.where(line == 1, weight_b, jnp.where(line == 2, slot_a, slot_b)),
        )
        small = contract_last(eye, small, HIGHEST)
        weight_a, weight_b = small[:, 0:1], small[:, 1:2]
        slot_col_a = small[:, 2:3].astype(jnp.int32)
        slot_col_b = small[:, 3:4].astype(jnp.int32)

    with scope("rows"):
        load("stream").wait()
        load("upstream").wait()
        inv_rms = jnp.zeros((tokens, 1), F32)
        for q in range(groups):
            piece = v["stream"][:, q * column : (q + 1) * column].astype(F32)
            inv_rms = inv_rms + jnp.sum(piece * piece, axis=1, keepdims=True)
        inv_rms = lax.rsqrt(inv_rms / width + EPS)

        def quarter(q):
            return pl.ds(start_of(q, column), column)

        def routed(cols, rows):
            normed = (v["stream"][:, cols].astype(F32) * inv_rms * v["gain"][:, cols]).astype(BF16)
            up = v["upstream"][:, cols].astype(F32)
            scaled_a = (weight_a * up).astype(BF16)
            scaled_b = (weight_b * up).astype(BF16)
            one, two = r["first"][rows], r["second"][rows]
            return (
                dot(one + two, normed).astype(BF16),
                (dot(one, scaled_a) + dot(two, scaled_b)).astype(BF16),
            )

        mine_q = quarter(tp)
        side = lax.rem(tp, 2)

        def lane_q(h):
            return quarter(side + 2 * h)

        def stage(cols, lo, hi, at, rows_to, cots_to):
            out_rows, out_cots = routed(cols, slice(lo * pcap, hi * pcap))
            rows_to[at] = out_rows
            cots_to[at] = out_cots

        for h in range(half):
            at = (slice(0, (near - 1) * pcap), slice(h * column, (h + 1) * column))
            stage(lane_q(h), 1, near, at, r["near_rows"], r["near_cots"])

    pairs = ((r["send_rows"], r["rows"]), (r["send_cots"], r["cots"]))
    close = (r["near_rows"], r["near_cots"])

    def block(m):
        return pl.ds(start_of(m, pcap), pcap)

    def near_copy(a, m, h):
        return remote(
            close[a].at[block(m - 1), pl.ds(h * column, column)],
            pairs[a][1].at[block(m), lane_q(h)],
            r["near_send"].at[a],
            r["near_recv"].at[a, m],
            {"sp": peer(m)},
        )

    def core_share(a, m, h):
        ref = pairs[a][1].at[block(m), lane_q(h)]
        return remote(
            ref, ref, r["share_send"].at[a], r["share_recv"].at[m], {"tp": flip(tp, 1)}
        )

    def sp_copy(a, m):
        src, full = pairs[a]
        return remote(
            src.at[block(m - near)],
            full.at[block(m), mine_q],
            r["sp_send"].at[a],
            r["sp_recv"].at[a, m - near],
            {"sp": peer(m)},
        )

    with scope("barrier"):
        pl.semaphore_wait(barrier, n - 1 + groups - 1)

    def send_near(m):
        for a in range(2):
            for h in range(half):
                near_copy(a, m, h).start()

    def send(m):
        for a in range(2):
            sp_copy(a, m).start()

    def send_any(lo, hi):
        each(lo, min(hi, near), send_near)
        each(max(lo, near), hi, send)

    send_any(1, n // 4)
    with scope("rows2"):
        stage(mine_q, near, n, slice(0, (n - near) * pcap), r["send_rows"], r["send_cots"])
    send_any(n // 2, 3 * n // 4)
    send_any(n // 4, n // 2)
    send_any(3 * n // 4, n)

    with scope("stats"):
        load("filtered").wait()
        filt = v["filtered"][...]
        square = filt.astype(F32) * filt.astype(F32)
        high = square.astype(BF16)
        low = (square - high.astype(F32)).astype(BF16)
        ones = jnp.ones((8, here), BF16)
        total = contract_last(ones, filt)
        total_square = contract_last(ones, high) + contract_last(ones, low)
        r["stats"][tp] = jnp.where(line == 0, total, total_square)
        sums = Direct(
            lambda o: r["stats"].at[o],
            tp,
            groups,
            r["st_send"],
            r["st_recv"],
            r["stats"].at[pl.ds(0, groups - 1)],
        )
        sums.begin()

    with scope("own"):
        for q in range(groups):
            cols = slice(q * column, (q + 1) * column)
            own_rows, own_cots = routed(cols, slice(0, pcap))
            r["rows"][0:pcap, cols] = own_rows
            r["cots"][0:pcap, cols] = own_cots
        lane = lax.broadcasted_iota(jnp.int32, (tokens, slots), 1)
        r["places"][...] = (
            ((lane == slot_col_a) | (lane == slot_col_b)).astype(F32).astype(BF16)
        )

    def gather(a, m):
        return Spread(
            "tp",
            lambda o: pairs[a][1].at[block(m), quarter(o)],
            tp,
            groups,
            r["tp_send"].at[a],
            lambda k: r["tp_recv"].at[a, m - near, k],
            r["tp_last"].at[m - near],
        )

    def arrive_near(m):
        for a in range(2):
            ref = pairs[a][1].at[block(m), pl.ds(0, half * column)]
            remote(
                ref, ref, r["near_send"].at[a], r["near_recv"].at[a, m], {"sp": peer(m)}
            ).wait_recv()
            for h in range(half):
                core_share(a, m, h).start()

    def arrived_near(m):
        ref = r["rows"].at[block(m)]
        remote(
            ref, ref, r["share_send"].at[0], r["share_recv"].at[m], {"tp": flip(tp, 1)}
        ).wait_recv()

    def arrive(m):
        for a in range(2):
            sp_copy(a, m).wait_recv()
            gather(a, m).begin()

    def relay(m):
        for a in range(2):
            gather(a, m).relay()

    def arrived(m):
        gather(0, m).arrived(r["rows"].at[block(m)])

    def band(c):
        return pl.ds(bands[c][0] * pcap, (bands[c][1] - bands[c][0]) * pcap)

    wide = 2 * v["gate_w"].shape[1]
    turned = wide // 2

    def turn():
        tile = min(256, width)
        for t in range(0, width, tile):
            at = slice(t, t + tile)
            for k, name in enumerate(("gate_w", "up_w")):
                r["back_w"][k * turned : (k + 1) * turned, at] = v[name][at].T
            r["down_t"][at] = v["down_w"][:, at].T
            r["mixer_t"][at] = v["mixer"][:, at].T

    def compute(c):
        at = band(c)
        rows, cots = r["rows"][at], r["cots"][at]
        pre_gate = dot(rows, v["gate_w"][...])
        pre_up = dot(rows, v["up_w"][...])
        grad_hidden = dot(cots, r["down_t"][...])
        sigma = jax.nn.sigmoid(pre_gate)
        silu_gate = pre_gate * sigma
        grad_pre_gate = (grad_hidden * pre_up * silu_slope(pre_gate, sigma)).astype(BF16)
        grad_pre_up = (grad_hidden * silu_gate).astype(BF16)
        r["hidden"][at] = (silu_gate * pre_up).astype(BF16)
        r["gpg"][at] = grad_pre_gate
        r["gpu"][at] = grad_pre_up
        slopes_in = jnp.concatenate([grad_pre_gate, grad_pre_up], axis=1)
        for q in range(groups):
            cols = slice(q * column, (q + 1) * column)
            r["partial"][at, cols] = dot(slopes_in, r["back_w"][:, cols]).astype(BF16)

    mate = flip(tp, 1)
    mine = tp // 2

    def core_copy(c, h):
        return remote(
            r["partial"].at[band(c), quarter(lax.rem(mate, 2) + 2 * h)],
            r["halves"].at[band(c), pl.ds(h * column, column)],
            r["core_send"],
            r["core_recv"].at[c],
            {"tp": mate},
        )

    def cross(c, k):
        return remote(
            r["passing"].at[band(c), quarter(flip(mine, k))],
            r["crossed"].at[band(c), pl.ds((k - 1) * column, column)],
            r["x_send"],
            r["x_recv"].at[c, k - 1],
            {"tp": flip(tp, 2 * k)},
        )

    def start_core(c):
        for h in range(half):
            core_copy(c, h).start()

    def add_core(c, cross_now=True):
        ref = r["halves"].at[band(c)]
        remote(ref, ref, r["core_send"], r["core_recv"].at[c], {"tp": mate}).wait_recv()
        for h in range(half):
            cols = pl.ds(h * column, column)
            own = r["partial"][band(c), quarter(lax.rem(tp, 2) + 2 * h)].astype(F32)
            r["passing"][band(c), cols] = (
                own + r["halves"][band(c), cols].astype(F32)
            ).astype(BF16)
        if cross_now:
            start_cross(c)

    def start_cross(c):
        for k in range(1, half):
            cross(c, k).start()

    span = column // 2

    def strip(t):
        return pl.ds(t * span, span)

    def home_copy(m, t):
        return remote(
            r["outgoing"].at[block(m), strip(t)],
            r["back"].at[block(m), strip(t)],
            r["home_send"],
            r["home_recv"].at[t],
            {"sp": peer(m)},
        )

    def add_cross(c):
        for k in range(1, half):
            cross(c, k).wait_recv()
        for t in range(2):
            at = pl.ds(start_of(2 * mine + t, span), span)
            total = r["passing"][band(c), at].astype(F32)
            for k in range(1, half):
                other = pl.ds((k - 1) * column + t * span, span)
                total = total + r["crossed"][band(c), other].astype(F32)
            r["outgoing"][band(c), strip(t)] = total.astype(BF16)
            each(max(1, bands[c][0]), bands[c][1], lambda m: home_copy(m, t).start())

    def act_rows(s):
        return pl.ds(start_of(s, tokens), tokens)

    acts = Spread(
        "sp",
        lambda o: r["act_all"].at[act_rows(o)],
        me,
        n,
        r["act_send"],
        lambda k: r["act_recv"].at[k],
        r["act_last"],
    )

    def early(bit):
        acts.copy(0, bit).start()

    def arrivals(lo, hi, base=None):
        base = max(lo if base is None else base, near)
        with scope("arrive#m=%d" % lo):
            each(lo, min(hi, near), arrive_near)

            def step(m):
                arrive(m)
                if isinstance(m, int):
                    if m > base:
                        relay(m - 1)
                else:
                    pl.when(m > base)(lambda: relay(m - 1))

            each(max(lo, near), hi, step)

    def lastrelay(hi):
        if hi > near:
            with scope("relay#m=%d" % (hi - 1)):
                relay(hi - 1)

    def whole(c):
        lo, hi = bands[c]
        with scope("finish#c=%d" % c):
            each(max(1, lo), min(hi, near), arrived_near)
            each(max(1, lo, near), hi, arrived)
        with scope("compute#c=%d" % c):
            compute(c)
            start_core(c)

    with scope("turn"):
        for name in ("gate_w", "up_w", "down_w", "mixer"):
            load(name).wait()
        turn()
    def addcore(c, cross_now=True):
        with scope("addcore#c=%d" % c):
            add_core(c, cross_now)

    def addcross(c):
        with scope("addcross#c=%d" % c):
            add_cross(c)

    def act_relay(masks):
        for mask in masks:
            onward = bits_below(low_bit(mask))
            if onward:
                acts.wait(mask)
                for bit in onward:
                    acts.copy(mask, bit).start()

    act_masks = acts.masks()
    last = len(bands) - 1
    one, two, mid, three, final = (bands[c][0] for c in range(1, 6))
    arrivals(1, one)
    lastrelay(one)
    whole(0)
    arrivals(two, mid)
    arrivals(mid, three, mid)
    addcore(0)
    lastrelay(mid)
    whole(2)
    lastrelay(three)
    addcore(2)
    whole(3)
    with scope("normact"):
        sums.arrived()
        moments = r["stats"][0]
        for o in range(1, groups):
            moments = moments + r["stats"][o]
        moments = contract_last(eye, moments, HIGHEST)
        mean_c = moments[:, 0:1] / channels
        variance = moments[:, 1:2] / channels - mean_c * mean_c
        inv_std = lax.rsqrt(variance + EPS)
        load("channel_gain").wait()

        def norms():
            centred = (v["filtered"][...].astype(F32) - mean_c) * inv_std
            normal_out = centred * v["channel_gain"][...]
            return centred, normal_out, jax.nn.sigmoid(normal_out)

        _, normal_out, sig_norm = norms()
        r["act_all"][act_rows(me)] = (normal_out * sig_norm).astype(BF16)

    addcore(3)
    addcross(0)
    arrivals(one, two)
    lastrelay(two)
    arrivals(three, final)
    whole(1)
    arrivals(final, n)
    addcross(2)
    addcore(1)
    addcross(3)
    for bit in bits_below(n):
        early(bit)
    lastrelay(final)
    whole(4)
    lastrelay(n)
    addcore(4)
    whole(5)
    addcross(1)
    addcore(5)
    addcross(4)
    with scope("actrelay1"):
        act_relay([m for m in act_masks if m < top])

    tile = min(256, width)

    def wgrad(left, pick, lo=0, hi=width // tile):
        def step(t):
            cols = pl.ds(start_of(t, tile), tile)
            r[pick][cols] = contract_first(r["rows"][:, cols], r[left][...])

        lax.fori_loop(lo, hi, lambda t, c: (step(t), c)[1], 0)

    def wgrad_down():
        def step(t):
            cols = pl.ds(start_of(t, tile), tile)
            r["out_down"][:, cols] = contract_first(r["hidden"][...], r["cots"][:, cols])

        lax.fori_loop(0, width // tile, lambda t, c: (step(t), c)[1], 0)

    with scope("wgrad_gate"):
        wgrad("gpg", "out_gate", 0, width // tile * 7 // 8)
    with scope("addcross#c=%d" % last):
        add_cross(last)
        r["back"][0:pcap] = r["outgoing"][0:pcap]
    with scope("actrelay2"):
        act_relay([top])
    with scope("wgrad_up"):
        wgrad("gpg", "out_gate", width // tile * 7 // 8, width // tile)
        wgrad("gpu", "out_up")
    with scope("norms"):
        centred, normal_out, sig_norm = norms()
        r["centred"][...] = centred
        r["bend"][...] = silu_slope(normal_out, sig_norm) * v["channel_gain"][...]
    def homes(t):
        ref = r["back"].at[pl.ds(pcap, slots - pcap), strip(t)]
        return remote(ref, ref, r["home_send"], r["home_recv"].at[t], {"sp": peer(1)})

    def normal(t):
        return Spread(
            "tp",
            lambda o: r["grad_normed"].at[:, pl.ds(start_of(2 * o + t, span), span)],
            tp,
            groups,
            r["gn_send"],
            lambda k: r["gn_recv"].at[t, k],
            r["gn_last"],
        )

    for t in range(2):
        with scope("home#t=%d" % t):
            homes(t).wait_recv()
        with scope("combine#t=%d" % t):
            r["grad_normed"][:, pl.ds(start_of(2 * tp + t, span), span)] = dot(
                r["places"][...], r["back"][:, strip(t)]
            ).astype(BF16)
            normal(t).begin()
    with scope("wgrad_down"):
        wgrad_down()
    with scope("actrelay3"):
        act_relay([m for m in act_masks if m > top])
    with scope("gather"):
        for t in range(2):
            normal(t).relay()
        normal(0).arrived(r["grad_normed"].at[:, pl.ds(0, half * column)])

    with scope("gradstream"):
        inner = jnp.zeros((tokens, 1), F32)
        for q in range(groups):
            at = slice(q * column, (q + 1) * column)
            weighted = r["grad_normed"][:, at].astype(F32) * v["gain"][:, at]
            inner = inner + jnp.sum(
                weighted * v["stream"][:, at].astype(F32), axis=1, keepdims=True
            )
        inner = inv_rms * inv_rms * inv_rms * (inner / width)
        for q in range(groups):
            at = slice(q * column, (q + 1) * column)
            weighted = r["grad_normed"][:, at].astype(F32) * v["gain"][:, at]
            r["grad_stream"][:, at] = (
                v["upstream"][:, at].astype(F32)
                + inv_rms * weighted
                - v["stream"][:, at].astype(F32) * inner
            ).astype(BF16)

    def part(s, o):
        start = pl.multiple_of(s * tokens + o * portion, portion)
        return r["grad_all"].at[pl.ds(start, portion)]

    def parts_of(count):
        return r["grad_all"].at[pl.ds(0, count * portion)]

    def rows_of(h):
        return pl.ds(pl.multiple_of((side + 2 * h) * portion, portion), portion)

    if db == pdb:

        def cut(j, h):
            return r["grad_stream"].at[rows_of(h), pl.ds(pl.multiple_of(j * db, db), db)]

        def own_cut():
            r["grad_all"][act_rows(me)] = r["grad_stream"][
                :, pl.ds(pl.multiple_of(me * db, db), db)
            ]
    else:

        def pick(j):
            where = lax.broadcasted_iota(jnp.int32, (width, pdb), 0)
            lane = lax.broadcasted_iota(jnp.int32, (width, pdb), 1)
            return ((where == lane + j * db) & (lane < db)).astype(F32).astype(BF16)

        def stage_cut(j):
            for h in range(half):
                r["staged"][j, h * portion : (h + 1) * portion] = dot(
                    r["grad_stream"][rows_of(h)], pick(j)
                ).astype(BF16)

        each(0, n, stage_cut)

        def cut(j, h):
            return r["staged"].at[j, pl.ds(start_of(h, portion), portion)]

        def own_cut():
            r["grad_all"][act_rows(me)] = dot(r["grad_stream"][...], pick(me)).astype(BF16)

    def cut_copy(m, h, j, s):
        return remote(
            cut(j, h), part(s, side + 2 * h), r["gs_send"], r["gs_recv"].at[m], {"sp": j}
        )

    def cut_sends_near(m):
        for h in range(half):
            cut_copy(m, h, peer(m), me).start()

    def spread_cut(m):
        s = peer(m)
        return Spread(
            "tp",
            lambda o: part(s, o),
            tp,
            groups,
            r["ga_send"],
            lambda k: r["ga_recv"].at[m, k],
            r["ga_last"],
        )

    def cut_arrives_near(m):
        ref = parts_of(half)
        remote(ref, ref, r["gs_send"], r["gs_recv"].at[m], {"sp": peer(m)}).wait_recv()
        for h in range(half):
            ref = part(peer(m), side + 2 * h)
            remote(ref, ref, r["ga_send"], r["ga_last"], {"tp": mate}).start()

    def cut_arrives(m):
        cut_copy(m, mine, peer(m), peer(m)).wait_recv()
        spread_cut(m).begin()

    with scope("cutstart"):
        each(near, n, lambda m: cut_copy(m, mine, peer(m), me).start())
        each(1, near, cut_sends_near)

    with scope("slopes"):
        grad_act = dot(r["grad_stream"][...], r["mixer_t"][...])
        centred = r["centred"][...]
        grad_centred = grad_act * r["bend"][...]
        ones = jnp.ones((8, here), F32)
        slope_sum = contract_last(ones, grad_centred, HIGHEST)
        slope_cross = contract_last(ones, grad_centred * centred, HIGHEST)
        r["slopes"][tp] = jnp.where(line == 0, slope_sum, slope_cross)
        meet = Direct(
            lambda o: r["slopes"].at[o],
            tp,
            groups,
            r["sl_send"],
            r["sl_recv"],
            r["slopes"].at[pl.ds(0, groups - 1)],
        )
        meet.begin()
        own_cut()
    with scope("meet"):
        meet.arrived()
    with scope("gradfiltered"):
        sums_b = r["slopes"][0]
        for o in range(1, groups):
            sums_b = sums_b + r["slopes"][o]
        sums_b = contract_last(eye, sums_b, HIGHEST)
        grad_filtered = (
            inv_std
            * (grad_centred - sums_b[:, 0:1] / channels - centred * (sums_b[:, 1:2] / channels))
        ).astype(BF16)
        r["halo_out"][...] = grad_filtered[:hpad]
        r["ext"][:tokens] = grad_filtered.astype(F32)

        def halo_copy():
            return remote(
                r["halo_out"], r["halo_in"], r["halo_send"], r["halo_recv"], {"sp": before}
            )

        halo_copy().start()

    def conv(lo, hi):
        mixed = jnp.zeros((hi - lo, here), F32)
        for k in range(reach + 1):
            mixed = mixed + v["taps"][k : k + 1] * r["ext"][lo + reach - k : hi + reach - k]
        sig_gate = jax.nn.sigmoid(v["gate"][lo:hi].astype(F32))
        r["out_value"][lo:hi] = (mixed * sig_gate).astype(BF16)
        r["out_gating"][lo:hi] = (
            mixed * v["value"][lo:hi].astype(F32) * sig_gate * (1.0 - sig_gate)
        ).astype(BF16)

    with scope("cutarrive2"):
        each(near, n, cut_arrives)
    with scope("cutarrive1"):
        each(1, near, cut_arrives_near)
    with scope("conv1"):
        for name in ("taps", "value", "gate"):
            load(name).wait()
        conv(0, tokens - hpad)
    with scope("halo"):
        halo_copy().wait_recv()
        inside = jnp.where(me < n - 1, 1.0, 0.0)
        r["ext"][tokens:] = r["halo_in"][...].astype(F32) * inside
    with scope("conv2"):
        conv(tokens - hpad, tokens)
    with scope("cutrelay"):
        each(near, n, lambda m: spread_cut(m).relay())
    with scope("cutwait"):
        spread_cut(1).arrived(parts_of((n - 1) * half))
    with scope("actwait"):
        acts.arrived(r["act_all"].at[pl.ds(0, n // 2 * tokens)])
    with scope("mixer"):
        r["out_mixer"][...] = contract_first(r["grad_all"][...], r["act_all"][...])[:db]

    with scope("drain"):

        def gone(ref, sem, where):
            remote(ref, ref, sem, r["halo_recv"], where).wait_send()

        sp_one, tp_one = {"sp": peer(1)}, {"tp": mate}
        far_rows = pl.ds(0, (n - near) * pcap)
        for a in range(2):
            gone(close[a], r["near_send"].at[a], sp_one)
            gone(close[a], r["share_send"].at[a], tp_one)
            gone(pairs[a][0], r["sp_send"].at[a], sp_one)
            ref = pairs[a][1].at[far_rows, pl.ds(0, (groups - 1) * column)]
            gone(ref, r["tp_send"].at[a], tp_one)
        gone(r["halves"], r["core_send"], tp_one)
        if half > 1:
            gone(r["crossed"], r["x_send"], tp_one)
        gone(r["back"].at[pl.ds(pcap, slots - pcap)], r["home_send"], sp_one)
        close_cuts, far_cuts = (near - 1) * half, n - near
        gone(parts_of(close_cuts + far_cuts), r["gs_send"], sp_one)
        gone(parts_of(close_cuts + far_cuts * (groups - 1)), r["ga_send"], tp_one)
        gone(r["act_all"].at[pl.ds(0, (n - 1) * tokens)], r["act_send"], sp_one)
        gone(r["grad_normed"].at[:, pl.ds(0, (groups - 1) * column)], r["gn_send"], tp_one)
        sums.sent()
        meet.sent()
        halo_copy().wait_send()


def flush_kernel(*refs):
    count = len(refs) // 2
    sems = refs[-1]
    copies = [
        pltpu.make_async_copy(refs[i], refs[count + i], sems.at[i]) for i in range(count)
    ]
    for copy in copies:
        copy.start()
    for copy in copies:
        copy.wait()


def body(
    stream,
    upstream,
    expert_gain,
    expert_ids,
    group_weight,
    pair_scores,
    gate_weight,
    up_weight,
    down_weight,
    mixer_weight,
    filtered,
    channel_gain,
    kernel_taps,
    value_branch,
    gate_branch,
):
    n, groups = lax.axis_size("sp"), lax.axis_size("tp")
    tokens, width = stream.shape
    capacity = max(2, 5 * tokens // (2 * n))
    pcap = round_up(capacity, 16)
    column = width // groups
    here = filtered.shape[1]
    hidden = gate_weight.shape[2]
    slots = n * pcap
    half = groups // 2
    db = width // n
    pdb = round_up(db, 128)
    hpad = round_up(kernel_taps.shape[0] - 1, 16)
    staged = (n, half * (tokens // groups), pdb) if pdb != db else (1, 16, 128)
    chunks = len(bands_of(n))
    near = direct_of(n)
    dma = pltpu.SemaphoreType.DMA
    shape = jax.ShapeDtypeStruct
    inputs = dict(
        ids=expert_ids.T,
        weight=group_weight[None],
        scores=pair_scores.T,
        gain=expert_gain[None],
        stream=stream,
        upstream=upstream,
        filtered=filtered,
        gate_w=gate_weight[0],
        up_w=up_weight[0],
        down_w=down_weight[0],
        channel_gain=channel_gain[None],
        mixer=mixer_weight,
        taps=kernel_taps,
        value=value_branch,
        gate=gate_branch,
    )
    outs = dict(
        out_value=shape((tokens, here), BF16),
        out_gating=shape((tokens, here), BF16),
        out_mixer=shape((db, here), F32),
        out_gate=shape((width, hidden), F32),
        out_up=shape((width, hidden), F32),
        out_down=shape((hidden, width), F32),
    )
    scratch = {"v_" + name: pltpu.VMEM(inputs[name].shape, inputs[name].dtype) for name in INPUTS}
    scratch |= dict(
        first=pltpu.VMEM((slots, tokens), BF16),
        second=pltpu.VMEM((slots, tokens), BF16),
        places=pltpu.VMEM((tokens, slots), BF16),
        send_rows=pltpu.VMEM((slots - near * pcap, column), BF16),
        send_cots=pltpu.VMEM((slots - near * pcap, column), BF16),
        near_rows=pltpu.VMEM(((near - 1) * pcap, half * column), BF16),
        near_cots=pltpu.VMEM(((near - 1) * pcap, half * column), BF16),
        rows=pltpu.VMEM((slots, width), BF16),
        cots=pltpu.VMEM((slots, width), BF16),
        hidden=pltpu.VMEM((slots, hidden), BF16),
        back_w=pltpu.VMEM((2 * hidden, width), BF16),
        down_t=pltpu.VMEM((width, hidden), BF16),
        mixer_t=pltpu.VMEM((width, here), BF16),
        centred=pltpu.VMEM((tokens, here), F32),
        bend=pltpu.VMEM((tokens, here), F32),
        gpg=pltpu.VMEM((slots, hidden), BF16),
        gpu=pltpu.VMEM((slots, hidden), BF16),
        partial=pltpu.VMEM((slots, width), BF16),
        halves=pltpu.VMEM((slots, half * column), BF16),
        passing=pltpu.VMEM((slots, half * column), BF16),
        crossed=pltpu.VMEM((slots, max(1, half - 1) * column), BF16),
        outgoing=pltpu.VMEM((slots, column), BF16),
        back=pltpu.VMEM((slots, column), BF16),
        grad_normed=pltpu.VMEM((tokens, width), BF16),
        grad_stream=pltpu.VMEM((tokens, width), BF16),
        staged=pltpu.VMEM(staged, BF16),
        grad_all=pltpu.VMEM((n * tokens, pdb), BF16),
        act_all=pltpu.VMEM((n * tokens, here), BF16),
        stats=pltpu.VMEM((groups, 8, tokens), F32),
        slopes=pltpu.VMEM((groups, 8, tokens), F32),
        halo_out=pltpu.VMEM((hpad, here), BF16),
        halo_in=pltpu.VMEM((hpad, here), BF16),
        ext=pltpu.VMEM((tokens + hpad, here), F32),
        load=dma((len(INPUTS),)),
    )
    middle = max(1, half - 1)
    for name, dims in dict(
        near_send=(2,),
        near_recv=(2, near),
        share_send=(2,),
        share_recv=(near,),
        sp_send=(2,),
        sp_recv=(2, n - near),
        tp_send=(2,),
        tp_recv=(2, n - near, middle),
        tp_last=(n - near,),
        st_send=(),
        st_recv=(),
        core_send=(),
        core_recv=(chunks,),
        x_send=(),
        x_recv=(chunks, middle),
        home_send=(),
        home_recv=(2,),
        gn_send=(),
        gn_recv=(2, middle),
        gn_last=(),
        act_send=(),
        act_recv=(n // 2 - 1,),
        act_last=(),
        gs_send=(),
        gs_recv=(n,),
        ga_send=(),
        ga_recv=(n, middle),
        ga_last=(),
        sl_send=(),
        sl_recv=(),
        halo_send=(),
        halo_recv=(),
    ).items():
        scratch[name] = dma(dims)
    names = (*INPUTS, *OUTPUTS, *scratch)
    vmem, hbm = pltpu.VMEM, pltpu.HBM
    results = pl.pallas_call(
        functools.partial(layer_kernel, n, groups, pcap, names),
        out_shape=[pltpu.VMEM(outs[name].shape, outs[name].dtype) for name in OUTPUTS],
        in_specs=[pl.BlockSpec(memory_space=hbm)] * len(INPUTS),
        out_specs=[pl.BlockSpec(memory_space=vmem)] * len(OUTPUTS),
        scratch_shapes=list(scratch.values()),
        compiler_params=pltpu.CompilerParams(
            collective_id=0, has_side_effects=True, vmem_limit_bytes=54 << 20
        ),
    )(*(inputs[name] for name in INPUTS))
    results = pl.pallas_call(
        flush_kernel,
        out_shape=[outs[name] for name in OUTPUTS],
        in_specs=[pl.BlockSpec(memory_space=vmem)] * len(OUTPUTS),
        out_specs=[pl.BlockSpec(memory_space=hbm)] * len(OUTPUTS),
        scratch_shapes=[dma((len(OUTPUTS),))],
        compiler_params=pltpu.CompilerParams(vmem_limit_bytes=1 << 20),
    )(*results)
    value, gating, mixer, gate, up, down = results
    return value, gating, mixer, gate[None], up[None], down[None]


def solution(mesh):
    return jax.shard_map(
        body,
        mesh=mesh,
        in_specs=(
            P("sp", None),
            P("sp", None),
            P(),
            P("sp", None),
            P("sp"),
            P("sp", None),
            P("sp", None, "tp"),
            P("sp", None, "tp"),
            P("sp", "tp", None),
            P("tp", None),
            P("sp", "tp"),
            P("tp"),
            P(None, "tp"),
            P("sp", "tp"),
            P("sp", "tp"),
        ),
        out_specs=(
            P("sp", "tp"),
            P("sp", "tp"),
            P("sp", "tp"),
            P("sp", None, "tp"),
            P("sp", None, "tp"),
            P("sp", "tp", None),
        ),
        check_vma=False,
    )
```

```python
import functools

import jax
import jax.numpy as jnp
from jax import lax
from jax.experimental import pallas as pl
from jax.experimental.pallas import tpu as pltpu
from jax.sharding import PartitionSpec as P

EPS = 1e-06
MESH = pl.DeviceIdType.MESH
F32 = jnp.float32
BF16 = jnp.bfloat16
HIGHEST = lax.Precision.HIGHEST
UNROLL = 8
DIRECT = 2


def silu_slope(value, sigma):
    return sigma * (1.0 + value * (1.0 - sigma))


def contract_last(left, right, precision=None):
    return lax.dot_general(
        left, right, (((1,), (1,)), ((), ())), preferred_element_type=F32, precision=precision
    )


def contract_first(left, right):
    return lax.dot_general(left, right, (((0,), (0,)), ((), ())), preferred_element_type=F32)


def dot(left, right):
    return jnp.dot(left, right, preferred_element_type=F32)


def round_up(value, unit):
    return -(-value // unit) * unit


def flip(index, mask):
    bit = 1
    while bit <= mask:
        if mask & bit:
            index = index + bit - 2 * bit * ((index // bit) % 2)
        bit *= 2
    return index


def either(index, mask, limit):
    if isinstance(mask, int):
        return flip(index, mask)
    bit, total = 1, 0
    while bit < limit:
        total = total + bit * (((index // bit) % 2 + (mask // bit) % 2) % 2)
        bit *= 2
    return total


def low_bit(mask):
    return mask & -mask


def bits_below(limit):
    found, bit = [], 1
    while bit < limit:
        found.append(bit)
        bit *= 2
    return found[::-1]


def remote(src, dst, send, recv, where):
    return pltpu.make_async_remote_copy(
        src_ref=src, dst_ref=dst, send_sem=send, recv_sem=recv, device_id=where, device_id_type=MESH
    )


def start_of(i, unit):
    return i * unit if isinstance(i, int) else pl.multiple_of(i * unit, unit)


class Spread:
    def __init__(self, axis, place, index, count, send, recv, last):
        self.axis, self.place, self.index, self.count = axis, place, index, count
        self.send_sem, self.recv, self.last = send, recv, last

    def recv_sem(self, mask):
        return self.last if mask % 2 else self.recv(mask // 2 - 1)

    def copy(self, mask, bit):
        ref = self.place(flip(self.index, mask))
        return remote(
            ref, ref, self.send_sem, self.recv_sem(mask | bit), {self.axis: flip(self.index, bit)}
        )

    def wait(self, mask):
        ref = self.place(flip(self.index, mask))
        where = {self.axis: flip(self.index, low_bit(mask))}
        remote(ref, ref, self.send_sem, self.recv_sem(mask), where).wait_recv()

    def begin(self):
        for bit in bits_below(self.count):
            self.copy(0, bit).start()

    def masks(self):
        return sorted(range(1, self.count), key=lambda m: (bin(m).count("1"), -low_bit(m)))

    def relay(self):
        for mask in self.masks():
            onward = bits_below(low_bit(mask))
            if onward:
                self.wait(mask)
                for bit in onward:
                    self.copy(mask, bit).start()

    def arrived(self, ref):
        where = {self.axis: flip(self.index, 1)}
        remote(ref, ref, self.send_sem, self.last, where).wait_recv()

    def sent(self, ref):
        where = {self.axis: flip(self.index, 1)}
        remote(ref, ref, self.send_sem, self.last, where).wait_send()


class Direct:
    def __init__(self, place, index, count, send, recv, others):
        self.place, self.index, self.count = place, index, count
        self.send_sem, self.recv_sem, self.others = send, recv, others

    def copy(self, ref, mask):
        return remote(ref, ref, self.send_sem, self.recv_sem, {"tp": flip(self.index, mask)})

    def begin(self):
        for mask in range(1, self.count):
            self.copy(self.place(self.index), mask).start()

    def arrived(self):
        self.copy(self.others, 1).wait_recv()

    def sent(self):
        self.copy(self.others, 1).wait_send()


def bands_of(n):
    sizes = (n // 4, n // 4, n // 8, n // 8, n // 8, n // 8)
    found, first = [], 0
    for size in sizes:
        found.append((first, first + size))
        first += size
    return found


def direct_of(n):
    return n // DIRECT


def each(first, last, step):
    if last - first <= UNROLL:
        for i in range(first, last):
            step(i)
        return

    def run(i, carry):
        step(i)
        return carry

    lax.fori_loop(first, last, run, 0)


INPUTS = (
    "ids",
    "weight",
    "scores",
    "gain",
    "stream",
    "upstream",
    "filtered",
    "gate_w",
    "up_w",
    "down_w",
    "channel_gain",
    "mixer",
    "taps",
    "value",
    "gate",
)
OUTPUTS = ("out_value", "out_gating", "out_mixer", "out_gate", "out_up", "out_down")


def layer_kernel(n, groups, pcap, names, *refs):
    r = dict(zip(names, refs))
    v = {name: r["v_" + name] for name in INPUTS}
    me, tp = lax.axis_index("sp"), lax.axis_index("tp")
    tokens, width = v["stream"].shape
    column = width // groups
    here = v["filtered"].shape[1]
    channels = here * groups
    slots = n * pcap
    portion = tokens // groups
    db = width // n
    pdb = r["grad_all"].shape[1]
    reach = v["taps"].shape[0] - 1
    hpad = r["halo_in"].shape[0]
    bands = bands_of(n)
    near = direct_of(n)
    top = n // 2
    half = groups // 2
    scope = jax.named_scope

    def peer(m):
        return either(me, m, n)

    barrier = pltpu.get_barrier_semaphore()
    each(
        1,
        n,
        lambda m: pl.semaphore_signal(
            barrier, inc=1, device_id={"sp": peer(m)}, device_id_type=MESH
        ),
    )
    for k in range(1, groups):
        pl.semaphore_signal(barrier, inc=1, device_id={"tp": flip(tp, k)}, device_id_type=MESH)
    before = lax.rem(me + n - 1, n)

    def load(name):
        return pltpu.make_async_copy(r[name], v[name], r["load"].at[INPUTS.index(name)])

    for name in INPUTS:
        load(name).start()

    with scope("slots"):
        earlier = (
            (
                lax.broadcasted_iota(jnp.int32, (tokens, tokens), 0)
                < lax.broadcasted_iota(jnp.int32, (tokens, tokens), 1)
            )
            .astype(F32)
            .astype(BF16)
        )
        eye = (
            lax.broadcasted_iota(jnp.int32, (tokens, tokens), 0)
            == lax.broadcasted_iota(jnp.int32, (tokens, tokens), 1)
        ).astype(F32)
        block_id = lax.broadcasted_iota(jnp.int32, (n, tokens), 0)
        expert = jnp.bitwise_xor(block_id, me)
        slot_at = lax.broadcasted_iota(jnp.int32, (slots, tokens), 0)
        load("ids").wait()
        hit_a = (expert == v["ids"][0:1]).astype(F32)
        hit_b = (expert == v["ids"][1:2]).astype(F32)
        ahead_a = dot(hit_a.astype(BF16), earlier)
        ahead_b = dot(hit_b.astype(BF16), earlier) + jnp.sum(hit_a, axis=1, keepdims=True)
        base = (block_id * pcap).astype(F32)
        slot_a = jnp.sum(hit_a * (ahead_a + base), axis=0, keepdims=True)
        slot_b = jnp.sum(hit_b * (ahead_b + base), axis=0, keepdims=True)
        first = (slot_at == slot_a.astype(jnp.int32)).astype(F32).astype(BF16)
        second = (slot_at == slot_b.astype(jnp.int32)).astype(F32).astype(BF16)
        both = first + second
        r["first"][...] = first
        r["second"][...] = second
        for name in ("weight", "scores", "gain"):
            load(name).wait()
        spread = v["scores"][0:1] - v["scores"][1:2]
        weight_a = v["weight"][...] * jax.nn.sigmoid(spread)
        weight_b = v["weight"][...] * jax.nn.sigmoid(-spread)
        line = lax.broadcasted_iota(jnp.int32, (8, tokens), 0)
        small = jnp.where(
            line == 0,
            weight_a,
            jnp.where(line == 1, weight_b, jnp.where(line == 2, slot_a, slot_b)),
        )
        small = contract_last(eye, small, HIGHEST)
        weight_a, weight_b = small[:, 0:1], small[:, 1:2]
        slot_col_a = small[:, 2:3].astype(jnp.int32)
        slot_col_b = small[:, 3:4].astype(jnp.int32)

    with scope("rows"):
        load("stream").wait()
        load("upstream").wait()
        inv_rms = jnp.zeros((tokens, 1), F32)
        for q in range(groups):
            piece = v["stream"][:, q * column : (q + 1) * column].astype(F32)
            inv_rms = inv_rms + jnp.sum(piece * piece, axis=1, keepdims=True)
        inv_rms = lax.rsqrt(inv_rms / width + EPS)

        def quarter(q):
            return pl.ds(start_of(q, column), column)

        def routed(cols, rows):
            normed = (v["stream"][:, cols].astype(F32) * inv_rms * v["gain"][:, cols]).astype(BF16)
            up = v["upstream"][:, cols].astype(F32)
            scaled_a = (weight_a * up).astype(BF16)
            scaled_b = (weight_b * up).astype(BF16)
            one, two = r["first"][rows], r["second"][rows]
            return (
                dot(one + two, normed).astype(BF16),
                (dot(one, scaled_a) + dot(two, scaled_b)).astype(BF16),
            )

        mine_q = quarter(tp)
        side = lax.rem(tp, 2)

        def lane_q(h):
            return quarter(side + 2 * h)

        def stage(cols, lo, hi, at, rows_to, cots_to):
            out_rows, out_cots = routed(cols, slice(lo * pcap, hi * pcap))
            rows_to[at] = out_rows
            cots_to[at] = out_cots

        for h in range(half):
            at = (slice(0, (near - 1) * pcap), slice(h * column, (h + 1) * column))
            stage(lane_q(h), 1, near, at, r["near_rows"], r["near_cots"])

    pairs = ((r["send_rows"], r["rows"]), (r["send_cots"], r["cots"]))
    close = (r["near_rows"], r["near_cots"])

    def block(m):
        return pl.ds(start_of(m, pcap), pcap)

    def near_copy(a, m, h):
        return remote(
            close[a].at[block(m - 1), pl.ds(h * column, column)],
            pairs[a][1].at[block(m), lane_q(h)],
            r["near_send"].at[a],
            r["near_recv"].at[a, m],
            {"sp": peer(m)},
        )

    def core_share(a, m, h):
        ref = pairs[a][1].at[block(m), lane_q(h)]
        return remote(
            ref, ref, r["share_send"].at[a], r["share_recv"].at[m], {"tp": flip(tp, 1)}
        )

    def sp_copy(a, m):
        src, full = pairs[a]
        return remote(
            src.at[block(m - near)],
            full.at[block(m), mine_q],
            r["sp_send"].at[a],
            r["sp_recv"].at[a, m - near],
            {"sp": peer(m)},
        )

    with scope("barrier"):
        pl.semaphore_wait(barrier, n - 1 + groups - 1)

    def send_near(m):
        for a in range(2):
            for h in range(half):
                near_copy(a, m, h).start()

    def send(m):
        for a in range(2):
            sp_copy(a, m).start()

    def send_any(lo, hi):
        each(lo, min(hi, near), send_near)
        each(max(lo, near), hi, send)

    send_any(1, n // 4)
    with scope("rows2"):
        stage(mine_q, near, n, slice(0, (n - near) * pcap), r["send_rows"], r["send_cots"])
    send_any(n // 2, 3 * n // 4)
    send_any(n // 4, n // 2)
    send_any(3 * n // 4, n)

    with scope("stats"):
        load("filtered").wait()
        filt = v["filtered"][...]
        square = filt.astype(F32) * filt.astype(F32)
        high = square.astype(BF16)
        low = (square - high.astype(F32)).astype(BF16)
        ones = jnp.ones((8, here), BF16)
        total = contract_last(ones, filt)
        total_square = contract_last(ones, high) + contract_last(ones, low)
        r["stats"][tp] = jnp.where(line == 0, total, total_square)
        sums = Direct(
            lambda o: r["stats"].at[o],
            tp,
            groups,
            r["st_send"],
            r["st_recv"],
            r["stats"].at[pl.ds(0, groups - 1)],
        )
        sums.begin()

    with scope("own"):
        for q in range(groups):
            cols = slice(q * column, (q + 1) * column)
            own_rows, own_cots = routed(cols, slice(0, pcap))
            r["rows"][0:pcap, cols] = own_rows
            r["cots"][0:pcap, cols] = own_cots
        lane = lax.broadcasted_iota(jnp.int32, (tokens, slots), 1)
        r["places"][...] = (
            ((lane == slot_col_a) | (lane == slot_col_b)).astype(F32).astype(BF16)
        )

    def gather(a, m):
        return Spread(
            "tp",
            lambda o: pairs[a][1].at[block(m), quarter(o)],
            tp,
            groups,
            r["tp_send"].at[a],
            lambda k: r["tp_recv"].at[a, m - near, k],
            r["tp_last"].at[m - near],
        )

    def arrive_near(m):
        for a in range(2):
            ref = pairs[a][1].at[block(m), pl.ds(0, half * column)]
            remote(
                ref, ref, r["near_send"].at[a], r["near_recv"].at[a, m], {"sp": peer(m)}
            ).wait_recv()
            for h in range(half):
                core_share(a, m, h).start()

    def arrived_near(m):
        ref = r["rows"].at[block(m)]
        remote(
            ref, ref, r["share_send"].at[0], r["share_recv"].at[m], {"tp": flip(tp, 1)}
        ).wait_recv()

    def arrive(m):
        for a in range(2):
            sp_copy(a, m).wait_recv()
            gather(a, m).begin()

    def relay(m):
        for a in range(2):
            gather(a, m).relay()

    def arrived(m):
        gather(0, m).arrived(r["rows"].at[block(m)])

    def band(c):
        return pl.ds(bands[c][0] * pcap, (bands[c][1] - bands[c][0]) * pcap)

    wide = 2 * v["gate_w"].shape[1]
    turned = wide // 2

    def turn():
        tile = min(256, width)
        for t in range(0, width, tile):
            at = slice(t, t + tile)
            for k, name in enumerate(("gate_w", "up_w")):
                r["back_w"][k * turned : (k + 1) * turned, at] = v[name][at].T
            r["down_t"][at] = v["down_w"][:, at].T
            r["mixer_t"][at] = v["mixer"][:, at].T

    def compute(c):
        at = band(c)
        rows, cots = r["rows"][at], r["cots"][at]
        pre_gate = dot(rows, v["gate_w"][...])
        pre_up = dot(rows, v["up_w"][...])
        grad_hidden = dot(cots, r["down_t"][...])
        sigma = jax.nn.sigmoid(pre_gate)
        silu_gate = pre_gate * sigma
        grad_pre_gate = (grad_hidden * pre_up * silu_slope(pre_gate, sigma)).astype(BF16)
        grad_pre_up = (grad_hidden * silu_gate).astype(BF16)
        r["hidden"][at] = (silu_gate * pre_up).astype(BF16)
        r["gpg"][at] = grad_pre_gate
        r["gpu"][at] = grad_pre_up
        slopes_in = jnp.concatenate([grad_pre_gate, grad_pre_up], axis=1)
        for q in range(groups):
            cols = slice(q * column, (q + 1) * column)
            r["partial"][at, cols] = dot(slopes_in, r["back_w"][:, cols]).astype(BF16)

    mate = flip(tp, 1)
    mine = tp // 2

    def core_copy(c, h):
        return remote(
            r["partial"].at[band(c), quarter(lax.rem(mate, 2) + 2 * h)],
            r["halves"].at[band(c), pl.ds(h * column, column)],
            r["core_send"],
            r["core_recv"].at[c],
            {"tp": mate},
        )

    def cross(c, k):
        return remote(
            r["passing"].at[band(c), quarter(flip(mine, k))],
            r["crossed"].at[band(c), pl.ds((k - 1) * column, column)],
            r["x_send"],
            r["x_recv"].at[c, k - 1],
            {"tp": flip(tp, 2 * k)},
        )

    def start_core(c):
        for h in range(half):
            core_copy(c, h).start()

    def add_core(c, cross_now=True):
        ref = r["halves"].at[band(c)]
        remote(ref, ref, r["core_send"], r["core_recv"].at[c], {"tp": mate}).wait_recv()
        for h in range(half):
            cols = pl.ds(h * column, column)
            own = r["partial"][band(c), quarter(lax.rem(tp, 2) + 2 * h)].astype(F32)
            r["passing"][band(c), cols] = (
                own + r["halves"][band(c), cols].astype(F32)
            ).astype(BF16)
        if cross_now:
            start_cross(c)

    def start_cross(c):
        for k in range(1, half):
            cross(c, k).start()

    span = column // 2

    def strip(t):
        return pl.ds(t * span, span)

    def home_copy(m, t):
        return remote(
            r["outgoing"].at[block(m), strip(t)],
            r["back"].at[block(m), strip(t)],
            r["home_send"],
            r["home_recv"].at[t],
            {"sp": peer(m)},
        )

    def add_cross(c):
        for k in range(1, half):
            cross(c, k).wait_recv()
        for t in range(2):
            at = pl.ds(start_of(2 * mine + t, span), span)
            total = r["passing"][band(c), at].astype(F32)
            for k in range(1, half):
                other = pl.ds((k - 1) * column + t * span, span)
                total = total + r["crossed"][band(c), other].astype(F32)
            r["outgoing"][band(c), strip(t)] = total.astype(BF16)
            each(max(1, bands[c][0]), bands[c][1], lambda m: home_copy(m, t).start())

    def act_rows(s):
        return pl.ds(start_of(s, tokens), tokens)

    acts = Spread(
        "sp",
        lambda o: r["act_all"].at[act_rows(o)],
        me,
        n,
        r["act_send"],
        lambda k: r["act_recv"].at[k],
        r["act_last"],
    )

    def early(bit):
        acts.copy(0, bit).start()

    def arrivals(lo, hi, base=None):
        base = max(lo if base is None else base, near)
        with scope("arrive#m=%d" % lo):
            each(lo, min(hi, near), arrive_near)

            def step(m):
                arrive(m)
                if isinstance(m, int):
                    if m > base:
                        relay(m - 1)
                else:
                    pl.when(m > base)(lambda: relay(m - 1))

            each(max(lo, near), hi, step)

    def lastrelay(hi):
        if hi > near:
            with scope("relay#m=%d" % (hi - 1)):
                relay(hi - 1)

    def whole(c):
        lo, hi = bands[c]
        with scope("finish#c=%d" % c):
            each(max(1, lo), min(hi, near), arrived_near)
            each(max(1, lo, near), hi, arrived)
        with scope("compute#c=%d" % c):
            compute(c)
            start_core(c)

    with scope("turn"):
        for name in ("gate_w", "up_w", "down_w", "mixer"):
            load(name).wait()
        turn()
    def addcore(c, cross_now=True):
        with scope("addcore#c=%d" % c):
            add_core(c, cross_now)

    def addcross(c):
        with scope("addcross#c=%d" % c):
            add_cross(c)

    def act_relay(masks):
        for mask in masks:
            onward = bits_below(low_bit(mask))
            if onward:
                acts.wait(mask)
                for bit in onward:
                    acts.copy(mask, bit).start()

    act_masks = acts.masks()
    last = len(bands) - 1
    one, two, mid, three, final = (bands[c][0] for c in range(1, 6))
    arrivals(1, one)
    lastrelay(one)
    whole(0)
    arrivals(two, mid)
    arrivals(mid, three, mid)
    addcore(0)
    lastrelay(mid)
    whole(2)
    lastrelay(three)
    addcore(2)
    whole(3)
    with scope("normact"):
        sums.arrived()
        moments = r["stats"][0]
        for o in range(1, groups):
            moments = moments + r["stats"][o]
        moments = contract_last(eye, moments, HIGHEST)
        mean_c = moments[:, 0:1] / channels
        variance = moments[:, 1:2] / channels - mean_c * mean_c
        inv_std = lax.rsqrt(variance + EPS)
        load("channel_gain").wait()

        def norms():
            centred = (v["filtered"][...].astype(F32) - mean_c) * inv_std
            normal_out = centred * v["channel_gain"][...]
            return centred, normal_out, jax.nn.sigmoid(normal_out)

        _, normal_out, sig_norm = norms()
        r["act_all"][act_rows(me)] = (normal_out * sig_norm).astype(BF16)

    addcore(3)
    addcross(0)
    arrivals(three, final)
    arrivals(one, two)
    lastrelay(two)
    whole(1)
    arrivals(final, n)
    addcross(2)
    addcore(1)
    addcross(3)
    for bit in bits_below(n):
        early(bit)
    lastrelay(final)
    whole(4)
    lastrelay(n)
    addcore(4)
    whole(5)
    addcross(1)
    addcore(5)
    addcross(4)
    with scope("actrelay1"):
        act_relay([m for m in act_masks if m < top])

    tile = min(256, width)

    def wgrad(left, pick, lo=0, hi=width // tile):
        def step(t):
            cols = pl.ds(start_of(t, tile), tile)
            r[pick][cols] = contract_first(r["rows"][:, cols], r[left][...])

        lax.fori_loop(lo, hi, lambda t, c: (step(t), c)[1], 0)

    def wgrad_down():
        def step(t):
            cols = pl.ds(start_of(t, tile), tile)
            r["out_down"][:, cols] = contract_first(r["hidden"][...], r["cots"][:, cols])

        lax.fori_loop(0, width // tile, lambda t, c: (step(t), c)[1], 0)

    with scope("wgrad_gate"):
        wgrad("gpg", "out_gate", 0, width // tile * 7 // 8)
    with scope("addcross#c=%d" % last):
        add_cross(last)
        r["back"][0:pcap] = r["outgoing"][0:pcap]
    with scope("actrelay2"):
        act_relay([top])
    with scope("wgrad_up"):
        wgrad("gpg", "out_gate", width // tile * 7 // 8, width // tile)
        wgrad("gpu", "out_up")
    with scope("norms"):
        centred, normal_out, sig_norm = norms()
        r["centred"][...] = centred
        r["bend"][...] = silu_slope(normal_out, sig_norm) * v["channel_gain"][...]
    def homes(t):
        ref = r["back"].at[pl.ds(pcap, slots - pcap), strip(t)]
        return remote(ref, ref, r["home_send"], r["home_recv"].at[t], {"sp": peer(1)})

    def normal(t):
        return Spread(
            "tp",
            lambda o: r["grad_normed"].at[:, pl.ds(start_of(2 * o + t, span), span)],
            tp,
            groups,
            r["gn_send"],
            lambda k: r["gn_recv"].at[t, k],
            r["gn_last"],
        )

    for t in range(2):
        with scope("home#t=%d" % t):
            homes(t).wait_recv()
        with scope("combine#t=%d" % t):
            r["grad_normed"][:, pl.ds(start_of(2 * tp + t, span), span)] = dot(
                r["places"][...], r["back"][:, strip(t)]
            ).astype(BF16)
            normal(t).begin()
    with scope("wgrad_down"):
        wgrad_down()
    with scope("actrelay3"):
        act_relay([m for m in act_masks if m > top])
    with scope("gather"):
        for t in range(2):
            normal(t).relay()
        normal(0).arrived(r["grad_normed"].at[:, pl.ds(0, half * column)])

    with scope("gradstream"):
        inner = jnp.zeros((tokens, 1), F32)
        for q in range(groups):
            at = slice(q * column, (q + 1) * column)
            weighted = r["grad_normed"][:, at].astype(F32) * v["gain"][:, at]
            inner = inner + jnp.sum(
                weighted * v["stream"][:, at].astype(F32), axis=1, keepdims=True
            )
        inner = inv_rms * inv_rms * inv_rms * (inner / width)
        for q in range(groups):
            at = slice(q * column, (q + 1) * column)
            weighted = r["grad_normed"][:, at].astype(F32) * v["gain"][:, at]
            r["grad_stream"][:, at] = (
                v["upstream"][:, at].astype(F32)
                + inv_rms * weighted
                - v["stream"][:, at].astype(F32) * inner
            ).astype(BF16)

    def part(s, o):
        start = pl.multiple_of(s * tokens + o * portion, portion)
        return r["grad_all"].at[pl.ds(start, portion)]

    def parts_of(count):
        return r["grad_all"].at[pl.ds(0, count * portion)]

    def rows_of(h):
        return pl.ds(pl.multiple_of((side + 2 * h) * portion, portion), portion)

    if db == pdb:

        def cut(j, h):
            return r["grad_stream"].at[rows_of(h), pl.ds(pl.multiple_of(j * db, db), db)]

        def own_cut():
            r["grad_all"][act_rows(me)] = r["grad_stream"][
                :, pl.ds(pl.multiple_of(me * db, db), db)
            ]
    else:

        def pick(j):
            where = lax.broadcasted_iota(jnp.int32, (width, pdb), 0)
            lane = lax.broadcasted_iota(jnp.int32, (width, pdb), 1)
            return ((where == lane + j * db) & (lane < db)).astype(F32).astype(BF16)

        def stage_cut(j):
            for h in range(half):
                r["staged"][j, h * portion : (h + 1) * portion] = dot(
                    r["grad_stream"][rows_of(h)], pick(j)
                ).astype(BF16)

        each(0, n, stage_cut)

        def cut(j, h):
            return r["staged"].at[j, pl.ds(start_of(h, portion), portion)]

        def own_cut():
            r["grad_all"][act_rows(me)] = dot(r["grad_stream"][...], pick(me)).astype(BF16)

    def cut_copy(m, h, j, s):
        return remote(
            cut(j, h), part(s, side + 2 * h), r["gs_send"], r["gs_recv"].at[m], {"sp": j}
        )

    def cut_sends_near(m):
        for h in range(half):
            cut_copy(m, h, peer(m), me).start()

    def spread_cut(m):
        s = peer(m)
        return Spread(
            "tp",
            lambda o: part(s, o),
            tp,
            groups,
            r["ga_send"],
            lambda k: r["ga_recv"].at[m, k],
            r["ga_last"],
        )

    def cut_arrives_near(m):
        ref = parts_of(half)
        remote(ref, ref, r["gs_send"], r["gs_recv"].at[m], {"sp": peer(m)}).wait_recv()
        for h in range(half):
            ref = part(peer(m), side + 2 * h)
            remote(ref, ref, r["ga_send"], r["ga_last"], {"tp": mate}).start()

    def cut_arrives(m):
        cut_copy(m, mine, peer(m), peer(m)).wait_recv()
        spread_cut(m).begin()

    with scope("cutstart"):
        each(near, n, lambda m: cut_copy(m, mine, peer(m), me).start())
        each(1, near, cut_sends_near)

    with scope("slopes"):
        grad_act = dot(r["grad_stream"][...], r["mixer_t"][...])
        centred = r["centred"][...]
        grad_centred = grad_act * r["bend"][...]
        ones = jnp.ones((8, here), F32)
        slope_sum = contract_last(ones, grad_centred, HIGHEST)
        slope_cross = contract_last(ones, grad_centred * centred, HIGHEST)
        r["slopes"][tp] = jnp.where(line == 0, slope_sum, slope_cross)
        meet = Direct(
            lambda o: r["slopes"].at[o],
            tp,
            groups,
            r["sl_send"],
            r["sl_recv"],
            r["slopes"].at[pl.ds(0, groups - 1)],
        )
        meet.begin()
        own_cut()
    with scope("meet"):
        meet.arrived()
    with scope("gradfiltered"):
        sums_b = r["slopes"][0]
        for o in range(1, groups):
            sums_b = sums_b + r["slopes"][o]
        sums_b = contract_last(eye, sums_b, HIGHEST)
        grad_filtered = (
            inv_std
            * (grad_centred - sums_b[:, 0:1] / channels - centred * (sums_b[:, 1:2] / channels))
        ).astype(BF16)
        r["halo_out"][...] = grad_filtered[:hpad]
        r["ext"][:tokens] = grad_filtered.astype(F32)

        def halo_copy():
            return remote(
                r["halo_out"], r["halo_in"], r["halo_send"], r["halo_recv"], {"sp": before}
            )

        halo_copy().start()

    def conv(lo, hi):
        mixed = jnp.zeros((hi - lo, here), F32)
        for k in range(reach + 1):
            mixed = mixed + v["taps"][k : k + 1] * r["ext"][lo + reach - k : hi + reach - k]
        sig_gate = jax.nn.sigmoid(v["gate"][lo:hi].astype(F32))
        r["out_value"][lo:hi] = (mixed * sig_gate).astype(BF16)
        r["out_gating"][lo:hi] = (
            mixed * v["value"][lo:hi].astype(F32) * sig_gate * (1.0 - sig_gate)
        ).astype(BF16)

    with scope("cutarrive2"):
        each(near, n, cut_arrives)
    with scope("conv1"):
        for name in ("taps", "value", "gate"):
            load(name).wait()
        conv(0, tokens - hpad)
    with scope("cutarrive1"):
        each(1, near, cut_arrives_near)
    with scope("halo"):
        halo_copy().wait_recv()
        inside = jnp.where(me < n - 1, 1.0, 0.0)
        r["ext"][tokens:] = r["halo_in"][...].astype(F32) * inside
    with scope("conv2"):
        conv(tokens - hpad, tokens)
    with scope("cutrelay"):
        each(near, n, lambda m: spread_cut(m).relay())
    with scope("cutwait"):
        spread_cut(1).arrived(parts_of((n - 1) * half))
    with scope("actwait"):
        acts.arrived(r["act_all"].at[pl.ds(0, n // 2 * tokens)])
    with scope("mixer"):
        r["out_mixer"][...] = contract_first(r["grad_all"][...], r["act_all"][...])[:db]

    with scope("drain"):

        def gone(ref, sem, where):
            remote(ref, ref, sem, r["halo_recv"], where).wait_send()

        sp_one, tp_one = {"sp": peer(1)}, {"tp": mate}
        far_rows = pl.ds(0, (n - near) * pcap)
        for a in range(2):
            gone(close[a], r["near_send"].at[a], sp_one)
            gone(close[a], r["share_send"].at[a], tp_one)
            gone(pairs[a][0], r["sp_send"].at[a], sp_one)
            ref = pairs[a][1].at[far_rows, pl.ds(0, (groups - 1) * column)]
            gone(ref, r["tp_send"].at[a], tp_one)
        gone(r["halves"], r["core_send"], tp_one)
        if half > 1:
            gone(r["crossed"], r["x_send"], tp_one)
        gone(r["back"].at[pl.ds(pcap, slots - pcap)], r["home_send"], sp_one)
        close_cuts, far_cuts = (near - 1) * half, n - near
        gone(parts_of(close_cuts + far_cuts), r["gs_send"], sp_one)
        gone(parts_of(close_cuts + far_cuts * (groups - 1)), r["ga_send"], tp_one)
        gone(r["act_all"].at[pl.ds(0, (n - 1) * tokens)], r["act_send"], sp_one)
        gone(r["grad_normed"].at[:, pl.ds(0, (groups - 1) * column)], r["gn_send"], tp_one)
        sums.sent()
        meet.sent()
        halo_copy().wait_send()


def flush_kernel(*refs):
    count = len(refs) // 2
    sems = refs[-1]
    copies = [
        pltpu.make_async_copy(refs[i], refs[count + i], sems.at[i]) for i in range(count)
    ]
    for copy in copies:
        copy.start()
    for copy in copies:
        copy.wait()


def body(
    stream,
    upstream,
    expert_gain,
    expert_ids,
    group_weight,
    pair_scores,
    gate_weight,
    up_weight,
    down_weight,
    mixer_weight,
    filtered,
    channel_gain,
    kernel_taps,
    value_branch,
    gate_branch,
):
    n, groups = lax.axis_size("sp"), lax.axis_size("tp")
    tokens, width = stream.shape
    capacity = max(2, 5 * tokens // (2 * n))
    pcap = round_up(capacity, 16)
    column = width // groups
    here = filtered.shape[1]
    hidden = gate_weight.shape[2]
    slots = n * pcap
    half = groups // 2
    db = width // n
    pdb = round_up(db, 128)
    hpad = round_up(kernel_taps.shape[0] - 1, 16)
    staged = (n, half * (tokens // groups), pdb) if pdb != db else (1, 16, 128)
    chunks = len(bands_of(n))
    near = direct_of(n)
    dma = pltpu.SemaphoreType.DMA
    shape = jax.ShapeDtypeStruct
    inputs = dict(
        ids=expert_ids.T,
        weight=group_weight[None],
        scores=pair_scores.T,
        gain=expert_gain[None],
        stream=stream,
        upstream=upstream,
        filtered=filtered,
        gate_w=gate_weight[0],
        up_w=up_weight[0],
        down_w=down_weight[0],
        channel_gain=channel_gain[None],
        mixer=mixer_weight,
        taps=kernel_taps,
        value=value_branch,
        gate=gate_branch,
    )
    outs = dict(
        out_value=shape((tokens, here), BF16),
        out_gating=shape((tokens, here), BF16),
        out_mixer=shape((db, here), F32),
        out_gate=shape((width, hidden), F32),
        out_up=shape((width, hidden), F32),
        out_down=shape((hidden, width), F32),
    )
    scratch = {"v_" + name: pltpu.VMEM(inputs[name].shape, inputs[name].dtype) for name in INPUTS}
    scratch |= dict(
        first=pltpu.VMEM((slots, tokens), BF16),
        second=pltpu.VMEM((slots, tokens), BF16),
        places=pltpu.VMEM((tokens, slots), BF16),
        send_rows=pltpu.VMEM((slots - near * pcap, column), BF16),
        send_cots=pltpu.VMEM((slots - near * pcap, column), BF16),
        near_rows=pltpu.VMEM(((near - 1) * pcap, half * column), BF16),
        near_cots=pltpu.VMEM(((near - 1) * pcap, half * column), BF16),
        rows=pltpu.VMEM((slots, width), BF16),
        cots=pltpu.VMEM((slots, width), BF16),
        hidden=pltpu.VMEM((slots, hidden), BF16),
        back_w=pltpu.VMEM((2 * hidden, width), BF16),
        down_t=pltpu.VMEM((width, hidden), BF16),
        mixer_t=pltpu.VMEM((width, here), BF16),
        centred=pltpu.VMEM((tokens, here), F32),
        bend=pltpu.VMEM((tokens, here), F32),
        gpg=pltpu.VMEM((slots, hidden), BF16),
        gpu=pltpu.VMEM((slots, hidden), BF16),
        partial=pltpu.VMEM((slots, width), BF16),
        halves=pltpu.VMEM((slots, half * column), BF16),
        passing=pltpu.VMEM((slots, half * column), BF16),
        crossed=pltpu.VMEM((slots, max(1, half - 1) * column), BF16),
        outgoing=pltpu.VMEM((slots, column), BF16),
        back=pltpu.VMEM((slots, column), BF16),
        grad_normed=pltpu.VMEM((tokens, width), BF16),
        grad_stream=pltpu.VMEM((tokens, width), BF16),
        staged=pltpu.VMEM(staged, BF16),
        grad_all=pltpu.VMEM((n * tokens, pdb), BF16),
        act_all=pltpu.VMEM((n * tokens, here), BF16),
        stats=pltpu.VMEM((groups, 8, tokens), F32),
        slopes=pltpu.VMEM((groups, 8, tokens), F32),
        halo_out=pltpu.VMEM((hpad, here), BF16),
        halo_in=pltpu.VMEM((hpad, here), BF16),
        ext=pltpu.VMEM((tokens + hpad, here), F32),
        load=dma((len(INPUTS),)),
    )
    middle = max(1, half - 1)
    for name, dims in dict(
        near_send=(2,),
        near_recv=(2, near),
        share_send=(2,),
        share_recv=(near,),
        sp_send=(2,),
        sp_recv=(2, n - near),
        tp_send=(2,),
        tp_recv=(2, n - near, middle),
        tp_last=(n - near,),
        st_send=(),
        st_recv=(),
        core_send=(),
        core_recv=(chunks,),
        x_send=(),
        x_recv=(chunks, middle),
        home_send=(),
        home_recv=(2,),
        gn_send=(),
        gn_recv=(2, middle),
        gn_last=(),
        act_send=(),
        act_recv=(n // 2 - 1,),
        act_last=(),
        gs_send=(),
        gs_recv=(n,),
        ga_send=(),
        ga_recv=(n, middle),
        ga_last=(),
        sl_send=(),
        sl_recv=(),
        halo_send=(),
        halo_recv=(),
    ).items():
        scratch[name] = dma(dims)
    names = (*INPUTS, *OUTPUTS, *scratch)
    vmem, hbm = pltpu.VMEM, pltpu.HBM
    results = pl.pallas_call(
        functools.partial(layer_kernel, n, groups, pcap, names),
        out_shape=[pltpu.VMEM(outs[name].shape, outs[name].dtype) for name in OUTPUTS],
        in_specs=[pl.BlockSpec(memory_space=hbm)] * len(INPUTS),
        out_specs=[pl.BlockSpec(memory_space=vmem)] * len(OUTPUTS),
        scratch_shapes=list(scratch.values()),
        compiler_params=pltpu.CompilerParams(
            collective_id=0, has_side_effects=True, vmem_limit_bytes=54 << 20
        ),
    )(*(inputs[name] for name in INPUTS))
    results = pl.pallas_call(
        flush_kernel,
        out_shape=[outs[name] for name in OUTPUTS],
        in_specs=[pl.BlockSpec(memory_space=vmem)] * len(OUTPUTS),
        out_specs=[pl.BlockSpec(memory_space=hbm)] * len(OUTPUTS),
        scratch_shapes=[dma((len(OUTPUTS),))],
        compiler_params=pltpu.CompilerParams(vmem_limit_bytes=1 << 20),
    )(*results)
    value, gating, mixer, gate, up, down = results
    return value, gating, mixer, gate[None], up[None], down[None]


def solution(mesh):
    return jax.shard_map(
        body,
        mesh=mesh,
        in_specs=(
            P("sp", None),
            P("sp", None),
            P(),
            P("sp", None),
            P("sp"),
            P("sp", None),
            P("sp", None, "tp"),
            P("sp", None, "tp"),
            P("sp", "tp", None),
            P("tp", None),
            P("sp", "tp"),
            P("tp"),
            P(None, "tp"),
            P("sp", "tp"),
            P("sp", "tp"),
        ),
        out_specs=(
            P("sp", "tp"),
            P("sp", "tp"),
            P("sp", "tp"),
            P("sp", None, "tp"),
            P("sp", None, "tp"),
            P("sp", "tp", None),
        ),
        check_vma=False,
    )
```
